1024 devices in a mesh: sp: 16 (over z), dp: 64 (over y, x, core).
Axes of the slice: x: 4, y: 8, z: 16, core: 2. Of those that a mesh axis runs over, the one named last changes fastest.
Arguments:
- mixing_input: bfloat16 [64, 2048, 2048], P('dp', 'sp'), may hold values from -6 to 6
- cotangent: bfloat16 [64, 2048, 2048], P('dp', 'sp'), may hold values from -6 to 6
- filter_taps: bfloat16 [4, 2048], P(None, 'sp'), may hold values from -3 to 3
- recurrence_gate_map: bfloat16 [2, 16, 128, 128], P(None, 'sp'), may hold values from -0.5 to 0.5
- input_gate_map: bfloat16 [2, 16, 128, 128], P(None, 'sp'), may hold values from -0.5 to 0.5
- decay_logit_param: float32 [2, 2048], P(None, 'sp')
- spike_decay: float32 [64, 16, 2048], P('dp', 'sp'), may hold values from -2 to -4.8828125e-05
Outputs:
- grad_input: bfloat16 [64, 2048, 2048], P('dp', 'sp')
- grad_rate_map: float32 [2, 16, 128, 128], P(None, 'sp')
- grad_input_map: float32 [2, 16, 128, 128], P(None, 'sp')
- grad_conv_taps: float32 [4, 2048], P(None, 'sp')
The draws below stay inside these ranges and needn't reach their ends.
All inputs are finite; a program needn't handle non-finite values.
Results may differ from the reference program's by a relative error of at most 0.0075.
Values may be sent and summed in bfloat16 or wider, within the bound.
A program may use at most 64 MiB of HBM per device.

```python
import math
import jax
import jax.numpy as jnp
from jax import lax

HEAD = 128
HEAD_COUNT = 16
CONV = 4
TOK_DEV = 128
WIDTH = 2048
SEQUENCE_LENGTH = 2048
BATCH_COUNT = 64


def draw_decay_logit_param(key, part):
    pick_key = jax.random.fold_in(key, 11)
    fast_key = jax.random.fold_in(key, 12)
    slow_key = jax.random.fold_in(key, 13)
    picked = jax.random.uniform(pick_key, (2, HEAD_COUNT, 1), jnp.float32)
    fast_heads = picked < 0.5
    fast_keep = jax.random.uniform(fast_key, (2, HEAD_COUNT, HEAD), jnp.float32, 0.004, 0.008)
    slow_keep = jax.random.uniform(slow_key, (2, HEAD_COUNT, HEAD), jnp.float32, 0.1, 0.4) / (4.0 * SEQUENCE_LENGTH)
    retain = jnp.where(fast_heads, fast_keep, slow_keep)
    return (-jnp.log(jnp.expm1(retain))).reshape(2, HEAD_COUNT * HEAD)


def draw_spike_decay(key, part):
    base_key = jax.random.fold_in(key, 21)
    position_key = jax.random.fold_in(key, 22)
    loss_key = jax.random.fold_in(key, 23)
    low_end = 0.25
    high_end = 1.0
    blocks = SEQUENCE_LENGTH // TOK_DEV
    baseline_rate = jnp.exp(jax.random.uniform(base_key, (BATCH_COUNT, HEAD_COUNT, blocks), jnp.float32, math.log(low_end), math.log(high_end))) / SEQUENCE_LENGTH
    baseline_rate = jnp.repeat(baseline_rate, TOK_DEV, axis=2)
    spike_positions = jax.random.randint(position_key, (BATCH_COUNT, HEAD_COUNT, 2), 0, SEQUENCE_LENGTH)
    loss_values = jax.random.uniform(loss_key, (BATCH_COUNT, HEAD_COUNT, 2), jnp.float32, 0.2, 0.5)
    position_index = jnp.arange(SEQUENCE_LENGTH)
    spike_events = spike_positions[:, :, :, None] == position_index[None, None, None, :]
    spike_total = jnp.sum(jnp.where(spike_events, jnp.log1p(-loss_values)[:, :, :, None], 0.0), axis=2)
    return spike_total - baseline_rate


def steps_of(stream_key, dims, split, least, high):
    def one(position, blocks):
        draws = jax.random.uniform(jax.random.fold_in(jax.random.fold_in(stream_key, 6), position), (blocks,), jnp.float32, least / len(split), high / len(split))
        return jnp.repeat(jnp.exp(draws), dims[position] // blocks).reshape((-1,) + (1,) * (len(dims) - position - 1))

    factor_of = one(*split[0])
    for cut in split[1:]:
        factor_of = factor_of * one(*cut)
    return factor_of


def gaussian(rng, dims, deviation, reach, split=(), kind=jnp.bfloat16):
    values = jax.random.normal(rng, dims, jnp.float32) * deviation
    if len(split) > 0:
        values = steps_of(rng, dims, split, -0.22, 0.18) * values
    return jnp.clip(values, min=-reach, max=reach).astype(kind)


def setup_inputs(seed: int = 0) -> dict:
    arg_keys = jax.random.split(jax.random.key(seed), 8)
    return {
        "mixing_input": gaussian(arg_keys[0], (BATCH_COUNT, SEQUENCE_LENGTH, WIDTH), 1.0, 6.0, ((0, 64), (1, 16))),
        "cotangent": gaussian(arg_keys[1], (BATCH_COUNT, SEQUENCE_LENGTH, WIDTH), 1.0, 6.0, ((0, 64), (1, 16))),
        "filter_taps": gaussian(arg_keys[2], (CONV, WIDTH), CONV ** -0.5, 3.0, ((1, 16),)),
        "recurrence_gate_map": gaussian(arg_keys[3], (2, HEAD_COUNT, HEAD, HEAD), HEAD ** -0.5, 0.5, ((1, 16),)),
        "input_gate_map": gaussian(arg_keys[4], (2, HEAD_COUNT, HEAD, HEAD), HEAD ** -0.5, 0.5, ((1, 16),)),
        "decay_logit_param": draw_decay_logit_param(jax.random.fold_in(arg_keys[7], 71), 0),
        "spike_decay": draw_spike_decay(jax.random.fold_in(arg_keys[7], 71), 0),
    }


decay_multiplier_value = 8.0

def forward_scan(coefficient, source):

    def combine(earlier, second):
        return (earlier[0] * second[0], second[0] * earlier[1] + second[1])
    return lax.associative_scan(combine, (coefficient, source), axis=0)[1]

def reverse_scan(coefficient, source):

    def combine(earlier, second):
        return (earlier[0] * second[0], second[0] * earlier[1] + second[1])
    return lax.associative_scan(combine, (coefficient, source), axis=0, reverse=True)[1]

def shift_down(signal):
    return jnp.concatenate([jnp.zeros_like(signal[:1]), signal[:-1]], axis=0)

def shift_up(signal):
    return jnp.concatenate([signal[1:], jnp.zeros_like(signal[:1])], axis=0)

def convolve(signal, kernel_taps):
    length = signal.shape[0]
    padded = jnp.pad(signal, ((2, 1), (0, 0), (0, 0)))
    running = padded[0:length] * kernel_taps[0]
    for offset in range(1, 4):
        running = running + padded[offset:offset + length] * kernel_taps[offset]
    return running

def convolve_back(signal, kernel_taps):
    length = signal.shape[0]
    padded = jnp.pad(signal, ((1, 2), (0, 0), (0, 0)))
    running = padded[3:3 + length] * kernel_taps[0]
    for offset in range(1, 4):
        running = running + padded[3 - offset:3 - offset + length] * kernel_taps[offset]
    return running

def tap_gradients(signal, value_grad):
    length = signal.shape[0]
    padded = jnp.pad(signal, ((2, 1), (0, 0), (0, 0)))
    return jnp.stack([lax.optimization_barrier(jnp.sum(padded[offset:offset + length] * value_grad, axis=0)) for offset in range(4)])

def directional_terms(lower_values, upstream_field, recurrence_weight, input_gate_weight, decay_logit_rows, spike_rows, backward_step):
    conv_values = lower_values.astype(jnp.float32)
    rate_wide = recurrence_weight.astype(jnp.float32)
    input_wide = input_gate_weight.astype(jnp.float32)
    recurrence_gate = jax.nn.sigmoid(jnp.einsum('thi,hij->thj', conv_values, rate_wide))
    input_gate = jax.nn.sigmoid(jnp.einsum('thi,hij->thj', conv_values, input_wide))
    logarithm_keep = jax.nn.log_sigmoid(decay_logit_rows)
    logarithm_decay = decay_multiplier_value * recurrence_gate * logarithm_keep + spike_rows[:, :, None]
    decay_factor = jnp.exp(logarithm_decay)
    multiplier = jnp.sqrt(-jnp.expm1(2.0 * logarithm_decay))
    source = multiplier * input_gate * conv_values
    if backward_step:
        hidden_state = reverse_scan(decay_factor, source)
        adjoint = forward_scan(shift_down(decay_factor), upstream_field)
        before = shift_up(hidden_state)
    else:
        hidden_state = forward_scan(decay_factor, source)
        adjoint = reverse_scan(shift_up(decay_factor), upstream_field)
        before = shift_down(hidden_state)
    log_grad = adjoint * before * decay_factor - adjoint * input_gate * conv_values * decay_factor * decay_factor / multiplier
    rate_back = lax.optimization_barrier((log_grad * decay_multiplier_value * logarithm_keep * recurrence_gate * (1.0 - recurrence_gate)).astype(jnp.bfloat16))
    gate_back = lax.optimization_barrier((adjoint * multiplier * conv_values * input_gate * (1.0 - input_gate)).astype(jnp.bfloat16))
    rate_back_wide = rate_back.astype(jnp.float32)
    gate_back_wide = gate_back.astype(jnp.float32)
    value_grad = adjoint * multiplier * input_gate
    value_grad = value_grad + jnp.einsum('thj,hij->thi', rate_back_wide, rate_wide)
    value_grad = value_grad + jnp.einsum('thj,hij->thi', gate_back_wide, input_wide)
    rate_gradient = jnp.einsum('thi,thj->hij', conv_values, rate_back_wide)
    gate_gradient = jnp.einsum('thi,thj->hij', conv_values, gate_back_wide)
    return (value_grad, rate_gradient, gate_gradient)

def reference(mixing_input, cotangent, filter_taps, recurrence_gate_map, input_gate_map, decay_logit_param, spike_decay):
    kernel_taps = filter_taps.astype(jnp.float32).reshape(CONV, HEAD_COUNT, HEAD)
    decay_logit_rows = decay_logit_param.reshape(2, HEAD_COUNT, HEAD)
    norm_factor = (BATCH_COUNT * SEQUENCE_LENGTH) ** (-0.5)

    def single_sequence(total_sums, sequence_items):
        input_rows, output_gradients, spike_values = sequence_items
        signal = input_rows.astype(jnp.float32).reshape(SEQUENCE_LENGTH, HEAD_COUNT, HEAD)
        lower_values = lax.optimization_barrier(convolve(signal, kernel_taps).astype(jnp.bfloat16))
        upstream_field = output_gradients.astype(jnp.float32).reshape(SEQUENCE_LENGTH, HEAD_COUNT, HEAD)
        spike_rows = jnp.transpose(spike_values)
        value_grad = jnp.zeros((SEQUENCE_LENGTH, HEAD_COUNT, HEAD), jnp.float32)
        rate_parts = []
        gate_parts = []
        for scan_direction in range(2):
            value_portion, rate_gradient, gate_gradient = directional_terms(lower_values, upstream_field, recurrence_gate_map[scan_direction], input_gate_map[scan_direction], decay_logit_rows[scan_direction], spike_rows, scan_direction == 1)
            value_grad = value_grad + value_portion
            rate_parts.append(rate_gradient)
            gate_parts.append(gate_gradient)
        input_grad = convolve_back(value_grad, kernel_taps).astype(jnp.bfloat16).reshape(SEQUENCE_LENGTH, HEAD_COUNT * HEAD)
        tap_part = tap_gradients(signal, value_grad)
        total_sums = (total_sums[0] + jnp.stack(rate_parts), total_sums[1] + jnp.stack(gate_parts), total_sums[2] + tap_part)
        return (total_sums, input_grad)
    starting_state = (jnp.zeros((2, HEAD_COUNT, HEAD, HEAD), jnp.float32), jnp.zeros((2, HEAD_COUNT, HEAD, HEAD), jnp.float32), jnp.zeros((CONV, HEAD_COUNT, HEAD), jnp.float32))
    total_sums, input_gradients = lax.scan(single_sequence, starting_state, (mixing_input, cotangent, spike_decay))
    return (input_gradients, total_sums[0] * norm_factor, total_sums[1] * norm_factor, (total_sums[2] * norm_factor).reshape(CONV, HEAD_COUNT * HEAD))
```

```python
import functools
import math

import jax
import jax.numpy as jnp
from jax import lax
from jax.experimental import pallas as pl
from jax.experimental.pallas import tpu as pltpu
from jax.sharding import PartitionSpec as P

MESH = pl.DeviceIdType.MESH
TB = 128
F32 = jnp.float32
BF16 = jnp.bfloat16
STRENGTH = 8.0


def grid_of(dp):
    return (8, 4, 2) if dp == 64 else (dp // 4, 2, 2)


def log_keep_of(logit):
    u = jnp.exp(-jnp.abs(logit))
    series = u * (1.0 - u * (0.5 - u * (1.0 / 3.0 - u * 0.25)))
    return jnp.minimum(logit, 0.0) - jnp.where(u < 0.01, series, jnp.log(1.0 + u))


def sigmoid(x):
    return 1.0 / (1.0 + jnp.exp(-x))


def one_less_square(log_decay, decay):
    y = -2.0 * log_decay
    series = y * (1.0 - y * (0.5 - y * (1.0 / 6.0 - y * (1.0 / 24.0 - y * (1.0 / 120.0)))))
    return jnp.where(y < 0.125, series, 1.0 - decay * decay)


def shifted(value, step, forward):
    return pltpu.roll(value, step if forward else 8 - step, 1)


def prefixes(coeff, row, forward):
    outs, product = [], coeff
    for step in (1, 2, 4):
        inside = (row >= step) if forward else (row < 8 - step)
        outs.append(jnp.where(inside, product, 0.0))
        product = jnp.where(inside, product * shifted(product, step, forward), product)
    return outs, product


def doubled(value, steps, forward):
    for step, coeff in zip((1, 2, 4), steps):
        value = value + coeff * shifted(value, step, forward)
    return value


def last_row(value, forward):
    edge = value[7:8] if forward else value[0:1]
    return jnp.broadcast_to(edge, value.shape)


def kernel(
    sizes,
    x_hbm,
    cot_hbm,
    taps_ref,
    wr_ref,
    wi_ref,
    logit_ref,
    spike_ref,
    gi_hbm,
    gr_ref,
    gm_ref,
    gt_ref,
    xr,
    cr,
    xf,
    vs,
    vt,
    wcat,
    pre,
    af,
    sc,
    e1,
    e2,
    c2,
    c3,
    qs,
    zs,
    vg,
    bk,
    go,
    halves,
    core_in,
    x_out,
    x_in,
    y_out,
    y_in,
    g2,
    g1,
    g0,
    local_sem,
    z_send,
    z_recv,
    o_send,
    o_recv,
    r_send,
    r_recv,
):
    n, ny, nx, nc, norm = sizes
    length = n * TB
    me = lax.axis_index("sp")
    dp = lax.axis_index("dp")
    core = lax.rem(dp, nc)
    xi = lax.rem(dp // nc, nx)
    yi = dp // (nc * nx)

    def at_plane(y, x, c):
        return {"sp": me, "dp": (y * nx + x) * nc + c}

    def along_z(peer):
        return {"sp": peer, "dp": dp}

    offsets = [n // 2]
    for d in range(n // 2 - 1, 0, -1):
        offsets += [d, n - d]
    x_peers = [lax.rem(xi + d, nx) for d in range(1, nx)]
    y_peers = [lax.rem(yi + d, ny) for d in range(1, ny)]
    partner = at_plane(yi, xi, 1 - core)

    barrier = pltpu.get_barrier_semaphore()
    greet = [along_z(lax.rem(me + d, n)) for d in offsets]
    greet += [at_plane(yi, x, core) for x in x_peers]
    greet += [at_plane(y, xi, core) for y in y_peers]
    greet += [partner]
    for device in greet:
        pl.semaphore_signal(barrier, inc=1, device_id=device, device_id_type=MESH)

    def columns(ref, block):
        return ref.at[0, :, pl.ds(pl.multiple_of(block * TB, TB), TB)]

    def rows_of(ref, block):
        return ref.at[pl.ds(pl.multiple_of(block * TB, TB), TB)]

    own = [
        pltpu.make_async_copy(columns(x_hbm, me), rows_of(xr, me), local_sem.at[0]),
        pltpu.make_async_copy(columns(cot_hbm, me), rows_of(cr, me), local_sem.at[1]),
    ]
    own[0].start()
    own[1].start()
    pl.semaphore_wait(barrier, len(greet))

    def inward(which, k):
        source, target = ((x_hbm, xr), (cot_hbm, cr))[which]
        peer = lax.rem(me + offsets[k], n)
        return pltpu.make_async_remote_copy(
            src_ref=columns(source, peer),
            dst_ref=rows_of(target, me),
            send_sem=z_send.at[which, k],
            recv_sem=z_recv.at[which, k],
            device_id=along_z(peer),
            device_id_type=MESH,
        )

    def arrived(which, k):
        source, target = ((x_hbm, xr), (cot_hbm, cr))[which]
        origin = lax.rem(me + n - offsets[k], n)
        pltpu.make_async_remote_copy(
            src_ref=columns(source, origin),
            dst_ref=rows_of(target, origin),
            send_sem=z_send.at[which, k],
            recv_sem=z_recv.at[which, k],
            device_id=along_z(origin),
            device_id_type=MESH,
        ).wait_recv()

    for which in range(2):
        for k in range(n - 1):
            inward(which, k).start()

    zero_rows = jnp.zeros((8, TB), F32)
    for ref in (xf, vg):
        ref[0:8, :] = zero_rows
        ref[length + 8 : length + 16, :] = zero_rows
    for d in range(2):
        af[d, 0:8, :] = zero_rows
        af[d, length + 8 : length + 16, :] = zero_rows
        wcat[:, 256 * d : 256 * d + 128] = wr_ref[d, 0]
        wcat[:, 256 * d + 128 : 256 * d + 256] = wi_ref[d, 0]
    taps = [taps_ref[k : k + 1, :].astype(F32) for k in range(4)]
    keep = [STRENGTH * log_keep_of(logit_ref[d : d + 1, :]) for d in range(2)]
    row = lax.broadcasted_iota(jnp.int32, (8, 8, TB), 1)
    row0 = lax.broadcasted_iota(jnp.int32, (8, TB), 0)

    own[0].wait()
    for k in range(n - 1):
        arrived(0, k)

    @pl.loop(0, n)
    def _(b):
        at = pl.multiple_of(b * TB, TB)
        xf[pl.ds(at + 8, TB), :] = xr[pl.ds(at, TB), :].astype(F32)

    @pl.loop(0, n)
    def _(b):
        at = pl.multiple_of(b * TB, TB)
        v = xf[pl.ds(at + 6, TB), :] * taps[0]
        for k in range(1, 4):
            v = v + xf[pl.ds(at + 6 + k, TB), :] * taps[k]
        low = v.astype(BF16)
        vs[pl.ds(at, TB), :] = low
        vt[:, pl.ds(at, TB)] = jnp.transpose(low.astype(F32)).astype(BF16)

    chunk = min(512, length)

    @pl.loop(0, length // chunk)
    def _(b):
        at = pl.multiple_of(b * chunk, chunk)
        pre[pl.ds(at, chunk), :] = jnp.dot(
            vs[pl.ds(at, chunk), :], wcat[...], preferred_element_type=F32
        )

    @pl.loop(0, n)
    def _(b):
        at = pl.multiple_of(b * TB, TB)
        spike = jnp.transpose(jnp.broadcast_to(spike_ref[pl.ds(b, 1), :], (TB, TB)))
        v = vs[pl.ds(at, TB), :].astype(F32)
        for d in range(2):
            rate = sigmoid(pre[pl.ds(at, TB), 256 * d : 256 * d + 128])
            gate = sigmoid(pre[pl.ds(at, TB), 256 * d + 128 : 256 * d + 256])
            log_decay = rate * keep[d] + spike
            decay = jnp.exp(log_decay)
            square = one_less_square(log_decay, decay)
            inverse = lax.rsqrt(square)
            multiplier = square * inverse
            gated = gate * v
            source = multiplier * gated
            slope = keep[d] * rate * (1.0 - rate)
            sloped = decay * slope
            af[d, pl.ds(at + 8, TB), :] = decay
            sc[d, pl.ds(at, TB), :] = source
            e1[d, pl.ds(at, TB), :] = sloped
            e2[d, pl.ds(at, TB), :] = -gated * decay * sloped * inverse
            c2[d, pl.ds(at, TB), :] = source * (1.0 - gate)
            c3[d, pl.ds(at, TB), :] = multiplier * gate

    def state_pass(d, block, carry):
        forward = d == 0
        at = pl.multiple_of(block * 64, 64)
        coeff = af[d, pl.ds(at + 8, 64), :].reshape(8, 8, TB)
        steps, product = prefixes(coeff, row, forward)
        value = doubled(sc[d, pl.ds(at, 64), :].reshape(8, 8, TB), steps, forward)
        for g in range(8) if forward else range(7, -1, -1):
            state = value[g] + product[g] * carry
            edge = (row0 == 0) if forward else (row0 == 7)
            before = jnp.where(edge, carry, pltpu.roll(state, 1 if forward else 7, 0))
            spot = pl.ds(at + 8 * g, 8)
            e1[d, spot, :] = before * e1[d, spot, :] + e2[d, spot, :]
            carry = last_row(state, forward)
        return carry

    def state_step(i, carry):
        ahead = state_pass(0, i, carry[0])
        back = state_pass(1, length // 64 - 1 - i, carry[1])
        return ahead, back

    start = jnp.zeros((8, TB), F32)
    lax.fori_loop(0, length // 64, state_step, (start, start))

    @pl.loop(0, length // 64)
    def _(i):
        at = pl.multiple_of(i * 64, 64)
        for d in range(2):
            forward = d == 1
            shift = -1 if forward else 1
            coeff = af[d, pl.ds(at + 8 + shift, 64), :].reshape(8, 8, TB)
            steps, product = prefixes(coeff, row, forward)
            for j, part in enumerate(steps + [product]):
                qs[d, j, pl.ds(at, 64), :] = part.reshape(64, TB)

    own[1].wait()
    for k in range(n - 1):
        arrived(1, k)

    def adjoint_pass(d, block, carry):
        forward = d == 1
        at = pl.multiple_of(block * 64, 64)
        steps = [qs[d, j, pl.ds(at, 64), :].reshape(8, 8, TB) for j in range(3)]
        value = cr[pl.ds(at, 64), :].astype(F32).reshape(8, 8, TB)
        value = doubled(value, steps, forward)
        product = qs[d, 3, pl.ds(at, 64), :].reshape(8, 8, TB)
        for g in range(8) if forward else range(7, -1, -1):
            adjoint = value[g] + product[g] * carry
            zs[d, pl.ds(at + 8 * g, 8), :] = adjoint
            carry = last_row(adjoint, forward)
        return carry

    def adjoint_step(i, carry):
        ahead = adjoint_pass(1, i, carry[0])
        back = adjoint_pass(0, length // 64 - 1 - i, carry[1])
        return ahead, back

    lax.fori_loop(0, length // 64, adjoint_step, (start, start))

    @pl.loop(0, length // 64)
    def _(i):
        at = pl.multiple_of(i * 64, 64)
        spot = pl.ds(at, 64)
        total = None
        for d in range(2):
            adjoint = zs[d, spot, :]
            bk[spot, 256 * d : 256 * d + 128] = (adjoint * e1[d, spot, :]).astype(BF16)
            bk[spot, 256 * d + 128 : 256 * d + 256] = (adjoint * c2[d, spot, :]).astype(BF16)
            part = adjoint * c3[d, spot, :]
            total = part if total is None else total + part
        vg[pl.ds(at + 8, 64), :] = total

    @pl.loop(0, length // chunk)
    def _(b):
        at = pl.multiple_of(b * chunk, chunk)
        vg[pl.ds(at + 8, chunk), :] += lax.dot_general(
            bk[pl.ds(at, chunk), :],
            wcat[...],
            (((1,), (1,)), ((), ())),
            preferred_element_type=F32,
        )

    def outward(block, k):
        return pltpu.make_async_remote_copy(
            src_ref=rows_of(go, block),
            dst_ref=columns(gi_hbm, me),
            send_sem=o_send.at[k],
            recv_sem=o_recv.at[k],
            device_id=along_z(block),
            device_id_type=MESH,
        )

    def input_grad(k, sums):
        block = lax.rem(me + k, n)
        at = pl.multiple_of(block * TB, TB)
        here = vg[pl.ds(at + 8, TB), :]
        total = here * taps[2]
        for j in (0, 1, 3):
            total = total + vg[pl.ds(at + 10 - j, TB), :] * taps[j]
        go[pl.ds(at, TB), :] = total.astype(BF16)

        @pl.when(k > 0)
        def _():
            outward(block, k).start()

        return tuple(
            sums[j]
            + jnp.sum((xf[pl.ds(at + 6 + j, TB), :] * here).reshape(TB // 8, 8, TB), axis=0)
            for j in range(4)
        )

    sums = lax.fori_loop(0, n, input_grad, (start,) * 4)
    own_out = pltpu.make_async_copy(rows_of(go, me), columns(gi_hbm, me), local_sem.at[2])
    own_out.start()

    maps = jnp.dot(vt[...], bk[...], preferred_element_type=F32)
    half = 512 // nc
    third = half // nx
    piece = third // ny
    tap_rows = [jnp.sum(s, axis=0, keepdims=True) for s in sums]
    tile = jnp.concatenate(tap_rows + [jnp.zeros((4, TB), F32)], axis=0)
    ordered = jnp.concatenate([maps[:, 128 * j : 128 * j + 128] for j in (0, 2, 1, 3)], axis=0)
    for c in range(nc):
        halves[c, 0:half, :] = ordered[half * c : half * (c + 1)]
        halves[c, half : half + 8, :] = tile

    def exchange(source, target, device, k):
        return pltpu.make_async_remote_copy(
            src_ref=source,
            dst_ref=target,
            send_sem=r_send.at[k],
            recv_sem=r_recv.at[k],
            device_id=device,
            device_id_type=MESH,
        )

    sent = []

    def stage(copies):
        for copy in copies:
            copy.start()
        sent.extend(copies)
        for copy in copies:
            copy.wait_recv()

    base = 0
    stage([exchange(halves.at[1 - core], core_in, partner, base)])
    base += 1
    mine = halves[pl.ds(core, 1)][0] + core_in[...]
    for j in range(nx):
        x_out[j, 0:third, :] = mine[third * j : third * (j + 1)]
        x_out[j, third : third + 8, :] = mine[half : half + 8]
    x_in[pl.ds(xi, 1)] = x_out[pl.ds(xi, 1)]
    stage(
        [
            exchange(x_out.at[p], x_in.at[xi], at_plane(yi, p, core), base + d)
            for d, p in enumerate(x_peers)
        ]
    )
    base += nx - 1
    mine = x_in[0]
    for j in range(1, nx):
        mine = mine + x_in[j]
    for j in range(ny):
        y_out[j, 0:piece, :] = mine[piece * j : piece * (j + 1)]
        y_out[j, piece : piece + 8, :] = mine[third : third + 8]
    y_in[pl.ds(yi, 1)] = y_out[pl.ds(yi, 1)]
    stage(
        [
            exchange(y_out.at[p], y_in.at[yi], at_plane(p, xi, core), base + d)
            for d, p in enumerate(y_peers)
        ]
    )
    base += ny - 1
    mine = y_in[0]
    for j in range(1, ny):
        mine = mine + y_in[j]
    mine = mine * norm
    gt_ref[...] = mine[piece : piece + 4]
    g2[pl.ds(yi, 1)] = mine[0:piece].reshape(1, piece, TB)
    stage(
        [
            exchange(g2.at[yi], g2.at[yi], at_plane(p, xi, core), base + d)
            for d, p in enumerate(y_peers)
        ]
    )
    base += ny - 1
    g1[pl.ds(xi, 1)] = g2[...].reshape(1, third, TB)
    stage(
        [
            exchange(g1.at[xi], g1.at[xi], at_plane(yi, p, core), base + d)
            for d, p in enumerate(x_peers)
        ]
    )
    base += nx - 1
    g0[pl.ds(core, 1)] = g1[...].reshape(1, half, TB)
    stage([exchange(g0.at[core], g0.at[core], partner, base)])
    whole = g0[...].reshape(512, TB)
    for d in range(2):
        gr_ref[d, 0] = whole[128 * d : 128 * d + 128]
        gm_ref[d, 0] = whole[256 + 128 * d : 384 + 128 * d]

    own_out.wait()
    for k in range(1, n):
        origin = lax.rem(me + n - k, n)
        pltpu.make_async_remote_copy(
            src_ref=rows_of(go, origin),
            dst_ref=columns(gi_hbm, origin),
            send_sem=o_send.at[k],
            recv_sem=o_recv.at[k],
            device_id=along_z(origin),
            device_id_type=MESH,
        ).wait_recv()
        outward(lax.rem(me + k, n), k).wait_send()
    for copy in sent:
        copy.wait_send()
    for which in range(2):
        for k in range(n - 1):
            inward(which, k).wait_send()


def body(sizes, x, cotangent, taps, rate_map, gate_map, logit, spike):
    n, ny, nx, nc, _ = sizes
    length = n * TB
    half, third, piece = 512 // nc, 512 // nc // nx, 512 // nc // nx // ny
    messages = 2 * (nc + nx + ny - 3)
    vmem, hbm = pl.BlockSpec(memory_space=pltpu.VMEM), pl.BlockSpec(memory_space=pl.ANY)
    grad_input, grad_rate, grad_gate, grad_taps = pl.pallas_call(
        functools.partial(kernel, sizes),
        name="recurrence_backward",
        out_shape=(
            jax.ShapeDtypeStruct(x.shape, BF16),
            jax.ShapeDtypeStruct(rate_map.shape, F32),
            jax.ShapeDtypeStruct(gate_map.shape, F32),
            jax.ShapeDtypeStruct(taps.shape, F32),
        ),
        in_specs=[hbm, hbm, vmem, vmem, vmem, vmem, vmem],
        out_specs=(hbm, vmem, vmem, vmem),
        scratch_shapes=[
            pltpu.VMEM((length, TB), BF16),
            pltpu.VMEM((length, TB), BF16),
            pltpu.VMEM((length + 16, TB), F32),
            pltpu.VMEM((length, TB), BF16),
            pltpu.VMEM((TB, length), BF16),
            pltpu.VMEM((TB, 512), BF16),
            pltpu.VMEM((length, 512), F32),
            pltpu.VMEM((2, length + 16, TB), F32),
            pltpu.VMEM((2, length, TB), F32),
            pltpu.VMEM((2, length, TB), F32),
            pltpu.VMEM((2, length, TB), F32),
            pltpu.VMEM((2, length, TB), F32),
            pltpu.VMEM((2, length, TB), F32),
            pltpu.VMEM((2, 4, length, TB), F32),
            pltpu.VMEM((2, length, TB), F32),
            pltpu.VMEM((length + 16, TB), F32),
            pltpu.VMEM((length, 512), BF16),
            pltpu.VMEM((length, TB), BF16),
            pltpu.VMEM((nc, half + 8, TB), F32),
            pltpu.VMEM((half + 8, TB), F32),
            pltpu.VMEM((nx, third + 8, TB), F32),
            pltpu.VMEM((nx, third + 8, TB), F32),
            pltpu.VMEM((ny, piece + 8, TB), F32),
            pltpu.VMEM((ny, piece + 8, TB), F32),
            pltpu.VMEM((ny, piece, TB), F32),
            pltpu.VMEM((nx, third, TB), F32),
            pltpu.VMEM((nc, half, TB), F32),
            pltpu.SemaphoreType.DMA((3,)),
            pltpu.SemaphoreType.DMA((2, n)),
            pltpu.SemaphoreType.DMA((2, n)),
            pltpu.SemaphoreType.DMA((n,)),
            pltpu.SemaphoreType.DMA((n,)),
            pltpu.SemaphoreType.DMA((messages,)),
            pltpu.SemaphoreType.DMA((messages,)),
        ],
        compiler_params=pltpu.CompilerParams(
            collective_id=0, has_side_effects=True, vmem_limit_bytes=60000 * 1024
        ),
    )(x, cotangent, taps, rate_map, gate_map, logit, spike.reshape(n, TB))
    return grad_input, grad_rate, grad_gate, grad_taps


def solution(mesh):
    n, dp = mesh.shape["sp"], mesh.shape["dp"]
    ny, nx, nc = grid_of(dp)
    sizes = (n, ny, nx, nc, 1.0 / math.sqrt(dp * n * TB))
    return jax.shard_map(
        functools.partial(body, sizes),
        mesh=mesh,
        in_specs=(
            P("dp", "sp", None),
            P("dp", "sp", None),
            P(None, "sp"),
            P(None, "sp", None, None),
            P(None, "sp", None, None),
            P(None, "sp"),
            P("dp", "sp", None),
        ),
        out_specs=(
            P("dp", "sp", None),
            P(None, "sp", None, None),
            P(None, "sp", None, None),
            P(None, "sp"),
        ),
        check_vma=False,
    )
```

```python
import functools
import math

import jax
import jax.numpy as jnp
from jax import lax
from jax.experimental import pallas as pl
from jax.experimental.pallas import tpu as pltpu
from jax.sharding import PartitionSpec as P

MESH = pl.DeviceIdType.MESH
TB = 128
F32 = jnp.float32
BF16 = jnp.bfloat16
STRENGTH = 8.0


def grid_of(dp):
    return (8, 4, 2) if dp == 64 else (dp // 4, 2, 2)


def log_keep_of(logit):
    u = jnp.exp(-jnp.abs(logit))
    series = u * (1.0 - u * (0.5 - u * (1.0 / 3.0 - u * 0.25)))
    return jnp.minimum(logit, 0.0) - jnp.where(u < 0.01, series, jnp.log(1.0 + u))


def sigmoid(x):
    return 1.0 / (1.0 + jnp.exp(-x))


def one_less_square(log_decay, decay):
    y = -2.0 * log_decay
    series = y * (1.0 - y * (0.5 - y * (1.0 / 6.0 - y * (1.0 / 24.0 - y * (1.0 / 120.0)))))
    return jnp.where(y < 0.125, series, 1.0 - decay * decay)


def shifted(value, step, forward):
    return pltpu.roll(value, step if forward else 8 - step, 1)


def prefixes(coeff, row, forward):
    outs, product = [], coeff
    for step in (1, 2, 4):
        inside = (row >= step) if forward else (row < 8 - step)
        outs.append(jnp.where(inside, product, 0.0))
        product = jnp.where(inside, product * shifted(product, step, forward), product)
    return outs, product


def doubled(value, steps, forward):
    for step, coeff in zip((1, 2, 4), steps):
        value = value + coeff * shifted(value, step, forward)
    return value


def last_row(value, forward):
    edge = value[7:8] if forward else value[0:1]
    return jnp.broadcast_to(edge, value.shape)


def kernel(
    sizes,
    x_hbm,
    cot_hbm,
    taps_hbm,
    wr_hbm,
    wi_hbm,
    logit_hbm,
    spike_hbm,
    gi_ref,
    gr_ref,
    gm_ref,
    gt_ref,
    taps_ref,
    wr_ref,
    wi_ref,
    logit_ref,
    spike_ref,
    xr,
    cr,
    xf,
    vs,
    vt,
    wcat,
    pre,
    af,
    sc,
    e1,
    e2,
    c2,
    c3,
    qs,
    gs,
    ends,
    carries,
    zs,
    vd,
    vg,
    bk,
    go,
    halves,
    core_in,
    x_out,
    x_in,
    y_out,
    y_in,
    g2,
    g1,
    g0,
    local_sem,
    small_sem,
    z_send,
    x_recv,
    c_recv,
    o_recv,
    r_send,
    r_recv,
):
    n, ny, nx, nc, norm = sizes
    length = n * TB
    me = lax.axis_index("sp")
    dp = lax.axis_index("dp")
    core = lax.rem(dp, nc)
    xi = lax.rem(dp // nc, nx)
    yi = dp // (nc * nx)

    def at_plane(y, x, c):
        return {"sp": me, "dp": (y * nx + x) * nc + c}

    def along_z(peer):
        return {"sp": peer, "dp": dp}

    offsets = [n // 2]
    for d in range(n // 2 - 1, 0, -1):
        offsets += [d, n - d]
    x_peers = [lax.rem(xi + d, nx) for d in range(1, nx)]
    y_peers = [lax.rem(yi + d, ny) for d in range(1, ny)]
    partner = at_plane(yi, xi, 1 - core)

    barrier = pltpu.get_barrier_semaphore()
    greet = [along_z(lax.rem(me + d, n)) for d in offsets]
    greet += [at_plane(yi, x, core) for x in x_peers]
    greet += [at_plane(y, xi, core) for y in y_peers]
    greet += [partner]
    for device in greet:
        pl.semaphore_signal(barrier, inc=1, device_id=device, device_id_type=MESH)

    def columns(ref, block):
        return ref.at[0, :, pl.ds(pl.multiple_of(block * TB, TB), TB)]

    def rows_of(ref, block):
        return ref.at[pl.ds(pl.multiple_of(block * TB, TB), TB)]

    own = [
        pltpu.make_async_copy(columns(x_hbm, me), rows_of(xr, me), local_sem.at[0]),
        pltpu.make_async_copy(columns(cot_hbm, me), rows_of(cr, me), local_sem.at[1]),
    ]
    own[0].start()
    own[1].start()
    small = [
        pltpu.make_async_copy(source, target, small_sem.at[j])
        for j, (source, target) in enumerate(
            (
                (taps_hbm, taps_ref),
                (wr_hbm, wr_ref),
                (wi_hbm, wi_ref),
                (logit_hbm, logit_ref),
                (spike_hbm, spike_ref),
            )
        )
    ]
    for copy in small:
        copy.start()
    pl.semaphore_wait(barrier, len(greet))

    def inward(which, k):
        source, target = ((x_hbm, xr), (cot_hbm, cr))[which]
        peer = lax.rem(me + offsets[k], n)
        return pltpu.make_async_remote_copy(
            src_ref=columns(source, peer),
            dst_ref=rows_of(target, me),
            send_sem=z_send,
            recv_sem=x_recv if which == 0 else c_recv.at[k],
            device_id=along_z(peer),
            device_id_type=MESH,
        )

    def cotangent_arrived(k):
        near = n // 2 - (k + 1) // 2
        origin = lax.rem(me + n - ((k % 2) * near + (1 - k % 2) * (n - near)), n)
        pltpu.make_async_copy(rows_of(cr, origin), rows_of(cr, origin), c_recv.at[k]).wait()
        return origin

    def wait_for_blocks(sem, count):
        rows = pl.ds(0, count * TB)
        pltpu.make_async_copy(xr.at[rows], xr.at[rows], sem).wait()

    for which in range(2):
        for k in range(n - 1):
            inward(which, k).start()

    for copy in small:
        copy.wait()
    zero_rows = jnp.zeros((8, TB), F32)
    xf[0:8, :] = zero_rows
    xf[length + 8 : length + 16, :] = zero_rows
    for edge in (0, length + 16):
        vd[edge : edge + 16, :] = jnp.zeros((16, TB), F32)
        bk[edge : edge + 16, :] = jnp.zeros((16, 512), BF16)
    for d in range(2):
        af[d, 0:8, :] = zero_rows
        af[d, length + 8 : length + 16, :] = zero_rows
        wcat[:, 256 * d : 256 * d + 128] = wr_ref[d, 0]
        wcat[:, 256 * d + 128 : 256 * d + 256] = wi_ref[d, 0]
    taps = [taps_ref[k : k + 1, :].astype(F32) for k in range(4)]
    keep = [STRENGTH * log_keep_of(logit_ref[d : d + 1, :]) for d in range(2)]
    row = lax.broadcasted_iota(jnp.int32, (8, 8, TB), 1)
    row0 = lax.broadcasted_iota(jnp.int32, (8, TB), 0)

    own[0].wait()
    wait_for_blocks(x_recv, n - 1)

    @pl.loop(0, n)
    def _(b):
        at = pl.multiple_of(b * TB, TB)
        xf[pl.ds(at + 8, TB), :] = xr[pl.ds(at, TB), :].astype(F32)

    @pl.loop(0, n)
    def _(b):
        at = pl.multiple_of(b * TB, TB)
        v = xf[pl.ds(at + 6, TB), :] * taps[0]
        for k in range(1, 4):
            v = v + xf[pl.ds(at + 6 + k, TB), :] * taps[k]
        low = v.astype(BF16)
        vs[pl.ds(at, TB), :] = low
        vt[:, pl.ds(at, TB)] = jnp.transpose(low.astype(F32)).astype(BF16)

    chunk = min(512, length)

    @pl.loop(0, length // chunk)
    def _(b):
        at = pl.multiple_of(b * chunk, chunk)
        pre[pl.ds(at, chunk), :] = jnp.dot(
            vs[pl.ds(at, chunk), :], wcat[...], preferred_element_type=F32
        )

    @pl.loop(0, n)
    def _(b):
        at = pl.multiple_of(b * TB, TB)
        spike = jnp.transpose(jnp.broadcast_to(spike_ref[pl.ds(b, 1), :], (TB, TB)))
        v = vs[pl.ds(at, TB), :].astype(F32)
        for d in range(2):
            rate = sigmoid(pre[pl.ds(at, TB), 256 * d : 256 * d + 128])
            gate = sigmoid(pre[pl.ds(at, TB), 256 * d + 128 : 256 * d + 256])
            log_decay = rate * keep[d] + spike
            decay = jnp.exp(log_decay)
            square = one_less_square(log_decay, decay)
            inverse = lax.rsqrt(square)
            multiplier = square * inverse
            gated = gate * v
            source = multiplier * gated
            slope = keep[d] * rate * (1.0 - rate)
            sloped = decay * slope
            af[d, pl.ds(at + 8, TB), :] = decay
            sc[d, pl.ds(at, TB), :] = source
            e1[d, pl.ds(at, TB), :] = sloped
            e2[d, pl.ds(at, TB), :] = -gated * decay * sloped * inverse
            c2[d, pl.ds(at, TB), :] = source * (1.0 - gate)
            c3[d, pl.ds(at, TB), :] = multiplier * gate

    def state_pass(d, block, carry):
        forward = d == 0
        at = pl.multiple_of(block * 64, 64)
        coeff = af[d, pl.ds(at + 8, 64), :].reshape(8, 8, TB)
        steps, product = prefixes(coeff, row, forward)
        value = doubled(sc[d, pl.ds(at, 64), :].reshape(8, 8, TB), steps, forward)
        for g in range(8) if forward else range(7, -1, -1):
            state = value[g] + product[g] * carry
            edge = (row0 == 0) if forward else (row0 == 7)
            before = jnp.where(edge, carry, pltpu.roll(state, 1 if forward else 7, 0))
            spot = pl.ds(at + 8 * g, 8)
            e1[d, spot, :] = before * e1[d, spot, :] + e2[d, spot, :]
            carry = last_row(state, forward)
        return carry

    def state_step(i, carry):
        ahead = state_pass(0, i, carry[0])
        back = state_pass(1, length // 64 - 1 - i, carry[1])
        return ahead, back

    start = jnp.zeros((8, TB), F32)
    lax.fori_loop(0, length // 64, state_step, (start, start))

    @pl.loop(0, n)
    def _(b):
        at = pl.multiple_of(b * TB, TB)
        for d in range(2):
            forward = d == 1
            shift = -1 if forward else 1
            carry = jnp.ones((8, TB), F32)
            for part in (0, 1) if forward else (1, 0):
                coeff = af[d, pl.ds(at + 64 * part + 8 + shift, 64), :].reshape(8, 8, TB)
                steps, product = prefixes(coeff, row, forward)
                for j, step in enumerate(steps):
                    qs[d, j, pl.ds(at + 64 * part, 64), :] = step.reshape(64, TB)
                qs[d, 3, pl.ds(at + 64 * part, 64), :] = product.reshape(64, TB)
                for g in range(8) if forward else range(7, -1, -1):
                    whole = product[g] * carry
                    gs[d, pl.ds(at + 64 * part + 8 * g, 8), :] = whole
                    carry = last_row(whole, forward)
            ends[d, 0, pl.ds(pl.multiple_of(b * 8, 8), 8), :] = carry

    def local_scan(d, block):
        forward = d == 1
        at = pl.multiple_of(block * TB, TB)
        carry = None
        for part in (0, 1) if forward else (1, 0):
            spot = pl.ds(at + 64 * part, 64)
            steps = [qs[d, j, spot, :].reshape(8, 8, TB) for j in range(3)]
            value = doubled(cr[spot, :].astype(F32).reshape(8, 8, TB), steps, forward)
            product = qs[d, 3, spot, :].reshape(8, 8, TB)
            for g in range(8) if forward else range(7, -1, -1):
                adjoint = value[g] if carry is None else value[g] + product[g] * carry
                zs[d, pl.ds(at + 64 * part + 8 * g, 8), :] = adjoint
                carry = last_row(adjoint, forward)
        ends[d, 1, pl.ds(pl.multiple_of(block * 8, 8), 8), :] = carry

    own[1].wait()
    local_scan(0, me)
    local_scan(1, me)

    @pl.loop(0, n - 1)
    def _(k):
        origin = cotangent_arrived(k)
        local_scan(0, origin)
        local_scan(1, origin)

    ahead = back = start
    for b in range(n):
        carries[1, 8 * b : 8 * b + 8, :] = ahead
        ahead = ends[1, 1, 8 * b : 8 * b + 8, :] + ends[1, 0, 8 * b : 8 * b + 8, :] * ahead
        r = n - 1 - b
        carries[0, 8 * r : 8 * r + 8, :] = back
        back = ends[0, 1, 8 * r : 8 * r + 8, :] + ends[0, 0, 8 * r : 8 * r + 8, :] * back

    @pl.loop(0, n)
    def _(b):
        incoming = [carries[d, pl.ds(pl.multiple_of(b * 8, 8), 8), :] for d in range(2)]
        for part in range(4):
            at = pl.multiple_of(b * TB + 32 * part, 32)
            spot, padded = pl.ds(at, 32), pl.ds(at + 16, 32)
            total = None
            for d in range(2):
                local = zs[d, spot, :].reshape(4, 8, TB)
                spread = gs[d, spot, :].reshape(4, 8, TB) * incoming[d][None]
                adjoint = (local + spread).reshape(32, TB)
                bk[padded, 256 * d : 256 * d + 128] = (adjoint * e1[d, spot, :]).astype(BF16)
                bk[padded, 256 * d + 128 : 256 * d + 256] = (adjoint * c2[d, spot, :]).astype(BF16)
                piece_of = adjoint * c3[d, spot, :]
                total = piece_of if total is None else total + piece_of
            vd[padded, :] = total

    def outward(block):
        return pltpu.make_async_remote_copy(
            src_ref=rows_of(go, block),
            dst_ref=columns(gi_ref, me),
            send_sem=z_send,
            recv_sem=o_recv,
            device_id=along_z(block),
            device_id_type=MESH,
        )

    group = max(1, n // 4)
    span = group * TB

    def input_grad(step, sums):
        turn = (1 - step // 2) * (2 + step) + (step // 2) * (3 - step)
        part = lax.rem(me // group + turn, n // group)
        base = pl.multiple_of(part * span, span)
        vg[...] = vd[pl.ds(base, span + 32), :] + lax.dot_general(
            bk[pl.ds(base, span + 32), :],
            wcat[...],
            (((1,), (1,)), ((), ())),
            preferred_element_type=F32,
        )
        for inner in range(group):
            block = part * group + inner
            at = pl.multiple_of(block * TB, TB)
            low = 16 + inner * TB
            here = vg[low : low + TB, :]
            total = here * taps[2]
            for j in (0, 1, 3):
                total = total + vg[low + 2 - j : low + 2 - j + TB, :] * taps[j]
            go[pl.ds(at, TB), :] = total.astype(BF16)

            @pl.when(block != me)
            def _(block=block):
                outward(block).start()

            sums = tuple(
                sums[j]
                + jnp.sum((xf[pl.ds(at + 6 + j, TB), :] * here).reshape(TB // 8, 8, TB), axis=0)
                for j in range(4)
            )
        return sums

    sums = lax.fori_loop(0, n // group, input_grad, (start,) * 4)
    own_out = pltpu.make_async_copy(rows_of(go, me), columns(gi_ref, me), local_sem.at[2])
    own_out.start()

    maps = jnp.dot(vt[...], bk[16 : length + 16, :], preferred_element_type=F32)
    half = 512 // nc
    third = half // nx
    piece = third // ny
    tap_rows = [jnp.sum(s, axis=0, keepdims=True) for s in sums]
    tile = jnp.concatenate(tap_rows + [jnp.zeros((4, TB), F32)], axis=0)
    ordered = jnp.concatenate([maps[:, 128 * j : 128 * j + 128] for j in (0, 2, 1, 3)], axis=0)
    for c in range(nc):
        halves[c, 0:half, :] = ordered[half * c : half * (c + 1)]
        halves[c, half : half + 8, :] = tile

    def exchange(source, target, device, k):
        return pltpu.make_async_remote_copy(
            src_ref=source,
            dst_ref=target,
            send_sem=r_send.at[k],
            recv_sem=r_recv.at[k],
            device_id=device,
            device_id_type=MESH,
        )

    sent = []

    def stage(copies):
        for copy in copies:
            copy.start()
        sent.extend(copies)
        for copy in copies:
            copy.wait_recv()

    base = 0
    stage([exchange(halves.at[1 - core], core_in, partner, base)])
    base += 1
    mine = halves[pl.ds(core, 1)][0] + core_in[...]
    for j in range(nx):
        x_out[j, 0:third, :] = mine[third * j : third * (j + 1)]
        x_out[j, third : third + 8, :] = mine[half : half + 8]
    x_in[pl.ds(xi, 1)] = x_out[pl.ds(xi, 1)]
    stage(
        [
            exchange(x_out.at[p], x_in.at[xi], at_plane(yi, p, core), base + d)
            for d, p in enumerate(x_peers)
        ]
    )
    base += nx - 1
    mine = x_in[0]
    for j in range(1, nx):
        mine = mine + x_in[j]
    for j in range(ny):
        y_out[j, 0:piece, :] = mine[piece * j : piece * (j + 1)]
        y_out[j, piece : piece + 8, :] = mine[third : third + 8]
    y_in[pl.ds(yi, 1)] = y_out[pl.ds(yi, 1)]
    stage(
        [
            exchange(y_out.at[p], y_in.at[yi], at_plane(p, xi, core), base + d)
            for d, p in enumerate(y_peers)
        ]
    )
    base += ny - 1
    mine = y_in[0]
    for j in range(1, ny):
        mine = mine + y_in[j]
    mine = mine * norm
    gt_ref[...] = mine[piece : piece + 4]
    g2[pl.ds(yi, 1)] = mine[0:piece].reshape(1, piece, TB)
    stage(
        [
            exchange(g2.at[yi], g2.at[yi], at_plane(p, xi, core), base + d)
            for d, p in enumerate(y_peers)
        ]
    )
    base += ny - 1
    g1[pl.ds(xi, 1)] = g2[...].reshape(1, third, TB)
    stage(
        [
            exchange(g1.at[xi], g1.at[xi], at_plane(yi, p, core), base + d)
            for d, p in enumerate(x_peers)
        ]
    )
    base += nx - 1
    g0[pl.ds(core, 1)] = g1[...].reshape(1, half, TB)
    stage([exchange(g0.at[core], g0.at[core], partner, base)])
    whole = g0[...].reshape(512, TB)
    for d in range(2):
        gr_ref[d, 0] = whole[128 * d : 128 * d + 128]
        gm_ref[d, 0] = whole[256 + 128 * d : 384 + 128 * d]

    own_out.wait()
    wait_for_blocks(o_recv, n - 1)
    for _ in range(3):
        wait_for_blocks(z_send, n - 1)
    for copy in sent:
        copy.wait_send()


def store(*refs):
    count = len(refs) // 2
    sems = refs[-1]
    copies = [
        pltpu.make_async_copy(refs[j], refs[count + j], sems.at[j]) for j in range(count)
    ]
    for copy in copies:
        copy.start()
    for copy in copies:
        copy.wait()


def body(sizes, x, cotangent, taps, rate_map, gate_map, logit, spike):
    n, ny, nx, nc, _ = sizes
    length = n * TB
    half, third, piece = 512 // nc, 512 // nc // nx, 512 // nc // nx // ny
    messages = 2 * (nc + nx + ny - 3)
    vmem, hbm = pl.BlockSpec(memory_space=pltpu.VMEM), pl.BlockSpec(memory_space=pl.ANY)
    results = pl.pallas_call(
        functools.partial(kernel, sizes),
        name="recurrence_backward",
        out_shape=(
            pltpu.VMEM(x.shape, BF16),
            pltpu.VMEM(rate_map.shape, F32),
            pltpu.VMEM(gate_map.shape, F32),
            pltpu.VMEM(taps.shape, F32),
        ),
        in_specs=[hbm] * 7,
        out_specs=(vmem,) * 4,
        scratch_shapes=[
            pltpu.VMEM(taps.shape, BF16),
            pltpu.VMEM(rate_map.shape, BF16),
            pltpu.VMEM(gate_map.shape, BF16),
            pltpu.VMEM(logit.shape, F32),
            pltpu.VMEM((n, TB), F32),
            pltpu.VMEM((length, TB), BF16),
            pltpu.VMEM((length, TB), BF16),
            pltpu.VMEM((length + 16, TB), F32),
            pltpu.VMEM((length, TB), BF16),
            pltpu.VMEM((TB, length), BF16),
            pltpu.VMEM((TB, 512), BF16),
            pltpu.VMEM((length, 512), F32),
            pltpu.VMEM((2, length + 16, TB), F32),
            pltpu.VMEM((2, length, TB), F32),
            pltpu.VMEM((2, length, TB), F32),
            pltpu.VMEM((2, length, TB), F32),
            pltpu.VMEM((2, length, TB), F32),
            pltpu.VMEM((2, length, TB), F32),
            pltpu.VMEM((2, 4, length, TB), F32),
            pltpu.VMEM((2, length, TB), F32),
            pltpu.VMEM((2, 2, 8 * n, TB), F32),
            pltpu.VMEM((2, 8 * n, TB), F32),
            pltpu.VMEM((2, length, TB), F32),
            pltpu.VMEM((length + 32, TB), F32),
            pltpu.VMEM((max(1, n // 4) * TB + 32, TB), F32),
            pltpu.VMEM((length + 32, 512), BF16),
            pltpu.VMEM((length, TB), BF16),
            pltpu.VMEM((nc, half + 8, TB), F32),
            pltpu.VMEM((half + 8, TB), F32),
            pltpu.VMEM((nx, third + 8, TB), F32),
            pltpu.VMEM((nx, third + 8, TB), F32),
            pltpu.VMEM((ny, piece + 8, TB), F32),
            pltpu.VMEM((ny, piece + 8, TB), F32),
            pltpu.VMEM((ny, piece, TB), F32),
            pltpu.VMEM((nx, third, TB), F32),
            pltpu.VMEM((nc, half, TB), F32),
            pltpu.SemaphoreType.DMA((3,)),
            pltpu.SemaphoreType.DMA((5,)),
            pltpu.SemaphoreType.DMA,
            pltpu.SemaphoreType.DMA,
            pltpu.SemaphoreType.DMA((n - 1,)),
            pltpu.SemaphoreType.DMA,
            pltpu.SemaphoreType.DMA((messages,)),
            pltpu.SemaphoreType.DMA((messages,)),
        ],
        compiler_params=pltpu.CompilerParams(
            collective_id=0, has_side_effects=True, vmem_limit_bytes=56 * 1024 * 1024
        ),
    )(x, cotangent, taps, rate_map, gate_map, logit, spike.reshape(n, TB))
    return pl.pallas_call(
        store,
        name="store_results",
        out_shape=tuple(jax.ShapeDtypeStruct(r.shape, r.dtype) for r in results),
        in_specs=[vmem] * 4,
        out_specs=(hbm,) * 4,
        scratch_shapes=[pltpu.SemaphoreType.DMA((4,))],
    )(*[pltpu.with_memory_space_constraint(r, pltpu.VMEM) for r in results])


def solution(mesh):
    n, dp = mesh.shape["sp"], mesh.shape["dp"]
    ny, nx, nc = grid_of(dp)
    sizes = (n, ny, nx, nc, 1.0 / math.sqrt(dp * n * TB))
    return jax.shard_map(
        functools.partial(body, sizes),
        mesh=mesh,
        in_specs=(
            P("dp", "sp", None),
            P("dp", "sp", None),
            P(None, "sp"),
            P(None, "sp", None, None),
            P(None, "sp", None, None),
            P(None, "sp"),
            P("dp", "sp", None),
        ),
        out_specs=(
            P("dp", "sp", None),
            P(None, "sp", None, None),
            P(None, "sp", None, None),
            P(None, "sp"),
        ),
        check_vma=False,
    )
```

```python
import functools
import math

import jax
import jax.numpy as jnp
from jax import lax
from jax.experimental import pallas as pl
from jax.experimental.pallas import tpu as pltpu
from jax.sharding import PartitionSpec as P

MESH = pl.DeviceIdType.MESH
TB = 128
F32 = jnp.float32
BF16 = jnp.bfloat16
STRENGTH = 8.0


def grid_of(dp):
    return (8, 4, 2) if dp == 64 else (dp // 4, 2, 2)


def log_keep_of(logit):
    u = jnp.exp(-jnp.abs(logit))
    series = u * (1.0 - u * (0.5 - u * (1.0 / 3.0 - u * 0.25)))
    return jnp.minimum(logit, 0.0) - jnp.where(u < 0.01, series, jnp.log(1.0 + u))


def sigmoid(x):
    return 1.0 / (1.0 + jnp.exp(-x))


def one_less_square(log_decay, decay):
    y = -2.0 * log_decay
    series = y * (1.0 - y * (0.5 - y * (1.0 / 6.0 - y * (1.0 / 24.0 - y * (1.0 / 120.0)))))
    return jnp.where(y < 0.125, series, 1.0 - decay * decay)


def shifted(value, step, forward):
    return pltpu.roll(value, step if forward else 8 - step, 1)


def prefixes(coeff, row, forward):
    outs, product = [], coeff
    for step in (1, 2, 4):
        inside = (row >= step) if forward else (row < 8 - step)
        outs.append(jnp.where(inside, product, 0.0))
        product = jnp.where(inside, product * shifted(product, step, forward), product)
    return outs, product


def doubled(value, steps, forward):
    for step, coeff in zip((1, 2, 4), steps):
        value = value + coeff * shifted(value, step, forward)
    return value


def last_row(value, forward):
    edge = value[7:8] if forward else value[0:1]
    return jnp.broadcast_to(edge, value.shape)


def kernel(
    sizes,
    x_hbm,
    cot_hbm,
    taps_hbm,
    wr_hbm,
    wi_hbm,
    logit_hbm,
    spike_hbm,
    gi_ref,
    gr_ref,
    gm_ref,
    gt_ref,
    taps_ref,
    wr_ref,
    wi_ref,
    logit_ref,
    spike_ref,
    xs,
    cs,
    xr,
    cr,
    xf,
    vs,
    vt,
    wcat,
    wt,
    pre,
    af,
    sc,
    e1,
    e2,
    c2,
    c3,
    qs,
    gs,
    ends,
    carries,
    zs,
    vd,
    vg,
    bk,
    go,
    halves,
    core_in,
    x_out,
    x_in,
    y_out,
    y_in,
    g2,
    g1,
    g0,
    local_sem,
    small_sem,
    z_send,
    x_recv,
    c_recv,
    o_recv,
    r_send,
    r_recv,
    joined,
):
    n, ny, nx, nc, norm = sizes
    length = n * TB
    me = lax.axis_index("sp")
    dp = lax.axis_index("dp")
    core = lax.rem(dp, nc)
    xi = lax.rem(dp // nc, nx)
    yi = dp // (nc * nx)

    def at_plane(y, x, c):
        return {"sp": me, "dp": (y * nx + x) * nc + c}

    def along_z(peer):
        return {"sp": peer, "dp": dp}

    offsets = [n // 2]
    for d in range(n // 2 - 1, 0, -1):
        offsets += [d, n - d]
    x_peers = [lax.rem(xi + d, nx) for d in range(1, nx)]
    y_peers = [lax.rem(yi + d, ny) for d in range(1, ny)]
    partner = at_plane(yi, xi, 1 - core)

    barrier = pltpu.get_barrier_semaphore()
    column = [along_z(lax.rem(me + d, n)) for d in offsets]
    plane = [at_plane(yi, x, core) for x in x_peers]
    plane += [at_plane(y, xi, core) for y in y_peers]
    plane += [partner]
    for device in column:
        pl.semaphore_signal(barrier, inc=1, device_id=device, device_id_type=MESH)

    @pl.when(me == 0)
    def _():
        for device in plane:
            pl.semaphore_signal(barrier, inc=1, device_id=device, device_id_type=MESH)

    def columns(ref, block):
        return ref.at[0, :, pl.ds(pl.multiple_of(block * TB, TB), TB)]

    def rows_of(ref, block):
        return ref.at[pl.ds(pl.multiple_of(block * TB, TB), TB)]

    own = [
        pltpu.make_async_copy(x_hbm.at[0], xs, local_sem.at[0]),
        pltpu.make_async_copy(cot_hbm.at[0], cs, local_sem.at[1]),
    ]
    own[0].start()
    own[1].start()
    small = [
        pltpu.make_async_copy(source, target, small_sem.at[j])
        for j, (source, target) in enumerate(
            (
                (taps_hbm, taps_ref),
                (wr_hbm, wr_ref),
                (wi_hbm, wi_ref),
                (logit_hbm, logit_ref),
                (spike_hbm, spike_ref),
            )
        )
    ]
    for copy in small:
        copy.start()

    @pl.when(me > 0)
    def _():
        pl.semaphore_wait(barrier, len(column))

    @pl.when(me == 0)
    def _():
        pl.semaphore_wait(barrier, len(column) + len(plane))


    def inward(which, k):
        source, target = ((xs, xr), (cs, cr))[which]
        peer = lax.rem(me + offsets[k], n)
        return pltpu.make_async_remote_copy(
            src_ref=source.at[:, pl.ds(pl.multiple_of(peer * TB, TB), TB)],
            dst_ref=rows_of(target, me),
            send_sem=z_send,
            recv_sem=x_recv if which == 0 else c_recv.at[(k + 1) // 2],
            device_id=along_z(peer),
            device_id_type=MESH,
        )

    def pair(j):
        near = n // 2 - j
        later = (j + n // 2 - 1) // (n // 2)
        return lax.rem(me + near, n), lax.rem(me + n - near * later, n)

    def wait_for_blocks(sem, count):
        rows = pl.ds(0, count * TB)
        pltpu.make_async_copy(xr.at[rows], xr.at[rows], sem).wait()

    mine = pl.ds(pl.multiple_of(me * TB, TB), TB)
    for which, (source, target) in enumerate(((xs, xr), (cs, cr))):
        own[which].wait()
        for k in range(n - 1):
            inward(which, k).start()
        target[mine, :] = source[:, mine]

    for copy in small:
        copy.wait()
    zero_rows = jnp.zeros((8, TB), F32)
    xf[0:8, :] = zero_rows
    xf[length + 8 : length + 16, :] = zero_rows
    for edge in (0, length + 16):
        vd[edge : edge + 16, :] = jnp.zeros((16, TB), F32)
        bk[edge : edge + 16, :] = jnp.zeros((16, 512), BF16)
    for d in range(2):
        af[d, 0:8, :] = zero_rows
        af[d, length + 8 : length + 16, :] = zero_rows
        wcat[:, 256 * d : 256 * d + 128] = wr_ref[d, 0]
        wcat[:, 256 * d + 128 : 256 * d + 256] = wi_ref[d, 0]
        for j, ref in enumerate((wr_ref, wi_ref)):
            flipped = jnp.transpose(ref[d, 0].astype(F32)).astype(BF16)
            wt[256 * d + 128 * j : 256 * d + 128 * j + 128, :] = flipped
    taps = [taps_ref[k : k + 1, :].astype(F32) for k in range(4)]
    keep = [STRENGTH * log_keep_of(logit_ref[d : d + 1, :]) for d in range(2)]
    row = lax.broadcasted_iota(jnp.int32, (8, 8, TB), 1)
    row0 = lax.broadcasted_iota(jnp.int32, (8, TB), 0)

    wait_for_blocks(x_recv, n - 1)

    @pl.when(me == 0)
    def _():
        for device in plane:
            pl.semaphore_signal(joined.at[0], inc=1, device_id=device, device_id_type=MESH)


    @pl.loop(0, n)
    def _(b):
        at = pl.multiple_of(b * TB, TB)
        xf[pl.ds(at + 8, TB), :] = xr[pl.ds(at, TB), :].astype(F32)

    @pl.loop(0, n)
    def _(b):
        at = pl.multiple_of(b * TB, TB)
        v = xf[pl.ds(at + 6, TB), :] * taps[0]
        for k in range(1, 4):
            v = v + xf[pl.ds(at + 6 + k, TB), :] * taps[k]
        low = v.astype(BF16)
        vs[pl.ds(at, TB), :] = low
        vt[:, pl.ds(at, TB)] = jnp.transpose(low.astype(F32)).astype(BF16)

    chunk = min(512, length)

    @pl.loop(0, length // chunk)
    def _(b):
        at = pl.multiple_of(b * chunk, chunk)
        pre[pl.ds(at, chunk), :] = jnp.dot(
            vs[pl.ds(at, chunk), :], wcat[...], preferred_element_type=F32
        )

    @pl.loop(0, n)
    def _(b):
        at = pl.multiple_of(b * TB, TB)
        spike = jnp.transpose(jnp.broadcast_to(spike_ref[pl.ds(b, 1), :], (TB, TB)))
        v = vs[pl.ds(at, TB), :].astype(F32)
        for d in range(2):
            rate = sigmoid(pre[pl.ds(at, TB), 256 * d : 256 * d + 128])
            gate = sigmoid(pre[pl.ds(at, TB), 256 * d + 128 : 256 * d + 256])
            log_decay = rate * keep[d] + spike
            decay = jnp.exp(log_decay)
            square = one_less_square(log_decay, decay)
            inverse = lax.rsqrt(square)
            multiplier = square * inverse
            gated = gate * v
            source = multiplier * gated
            slope = keep[d] * rate * (1.0 - rate)
            sloped = decay * slope
            af[d, pl.ds(at + 8, TB), :] = decay
            sc[d, pl.ds(at, TB), :] = source
            e1[d, pl.ds(at, TB), :] = sloped
            e2[d, pl.ds(at, TB), :] = -gated * decay * sloped * inverse
            c2[d, pl.ds(at, TB), :] = source * (1.0 - gate)
            c3[d, pl.ds(at, TB), :] = multiplier * gate

    def state_pass(d, block, carry):
        forward = d == 0
        at = pl.multiple_of(block * 64, 64)
        coeff = af[d, pl.ds(at + 8, 64), :].reshape(8, 8, TB)
        steps, product = prefixes(coeff, row, forward)
        value = doubled(sc[d, pl.ds(at, 64), :].reshape(8, 8, TB), steps, forward)
        for g in range(8) if forward else range(7, -1, -1):
            state = value[g] + product[g] * carry
            edge = (row0 == 0) if forward else (row0 == 7)
            before = jnp.where(edge, carry, pltpu.roll(state, 1 if forward else 7, 0))
            spot = pl.ds(at + 8 * g, 8)
            e1[d, spot, :] = before * e1[d, spot, :] + e2[d, spot, :]
            carry = last_row(state, forward)
        return carry

    def state_step(i, carry):
        ahead = state_pass(0, i, carry[0])
        back = state_pass(1, length // 64 - 1 - i, carry[1])
        return ahead, back

    start = jnp.zeros((8, TB), F32)
    lax.fori_loop(0, length // 64, state_step, (start, start))

    @pl.loop(0, n)
    def _(b):
        at = pl.multiple_of(b * TB, TB)
        for d in range(2):
            forward = d == 1
            shift = -1 if forward else 1
            carry = jnp.ones((8, TB), F32)
            for part in (0, 1) if forward else (1, 0):
                coeff = af[d, pl.ds(at + 64 * part + 8 + shift, 64), :].reshape(8, 8, TB)
                steps, product = prefixes(coeff, row, forward)
                for j, step in enumerate(steps):
                    qs[d, j, pl.ds(at + 64 * part, 64), :] = step.reshape(64, TB)
                qs[d, 3, pl.ds(at + 64 * part, 64), :] = product.reshape(64, TB)
                for g in range(8) if forward else range(7, -1, -1):
                    whole = product[g] * carry
                    gs[d, pl.ds(at + 64 * part + 8 * g, 8), :] = whole
                    carry = last_row(whole, forward)
            ends[d, 0, pl.ds(pl.multiple_of(b * 8, 8), 8), :] = carry

    def local_scan(d, block):
        forward = d == 1
        at = pl.multiple_of(block * TB, TB)
        carry = None
        for part in (0, 1) if forward else (1, 0):
            spot = pl.ds(at + 64 * part, 64)
            steps = [qs[d, j, spot, :].reshape(8, 8, TB) for j in range(3)]
            value = doubled(cr[spot, :].astype(F32).reshape(8, 8, TB), steps, forward)
            product = qs[d, 3, spot, :].reshape(8, 8, TB)
            for g in range(8) if forward else range(7, -1, -1):
                adjoint = value[g] if carry is None else value[g] + product[g] * carry
                zs[d, pl.ds(at + 64 * part + 8 * g, 8), :] = adjoint
                carry = last_row(adjoint, forward)
        ends[d, 1, pl.ds(pl.multiple_of(block * 8, 8), 8), :] = carry

    @pl.when(me == 0)
    def _():
        pl.semaphore_wait(joined.at[0], len(plane))
        for device in column:
            pl.semaphore_signal(joined.at[1], inc=1, device_id=device, device_id_type=MESH)

    def scan_pair(j):
        for block in pair(j):
            local_scan(0, block)
            local_scan(1, block)

    wait_for_blocks(c_recv.at[0], 1)
    scan_pair(0)

    @pl.loop(1, n // 2)
    def _(j):
        wait_for_blocks(c_recv.at[j], 2)
        scan_pair(j)

    ahead = back = start
    for b in range(n):
        carries[1, 8 * b : 8 * b + 8, :] = ahead
        ahead = ends[1, 1, 8 * b : 8 * b + 8, :] + ends[1, 0, 8 * b : 8 * b + 8, :] * ahead
        r = n - 1 - b
        carries[0, 8 * r : 8 * r + 8, :] = back
        back = ends[0, 1, 8 * r : 8 * r + 8, :] + ends[0, 0, 8 * r : 8 * r + 8, :] * back

    def finish_block(b):
        incoming = [carries[d, pl.ds(pl.multiple_of(b * 8, 8), 8), :] for d in range(2)]
        for part in range(4):
            at = pl.multiple_of(b * TB + 32 * part, 32)
            spot, padded = pl.ds(at, 32), pl.ds(at + 16, 32)
            total = None
            for d in range(2):
                local = zs[d, spot, :].reshape(4, 8, TB)
                spread = gs[d, spot, :].reshape(4, 8, TB) * incoming[d][None]
                adjoint = (local + spread).reshape(32, TB)
                bk[padded, 256 * d : 256 * d + 128] = (adjoint * e1[d, spot, :]).astype(BF16)
                bk[padded, 256 * d + 128 : 256 * d + 256] = (adjoint * c2[d, spot, :]).astype(BF16)
                direct = adjoint * c3[d, spot, :]
                total = direct if total is None else total + direct
            vd[padded, :] = total

    def outward(block):
        return pltpu.make_async_remote_copy(
            src_ref=rows_of(go, block),
            dst_ref=columns(gi_ref, me),
            send_sem=z_send,
            recv_sem=o_recv,
            device_id=along_z(block),
            device_id_type=MESH,
        )

    batch = min(4, n)

    def input_grad(blocks, sums):
        for i, block in enumerate(blocks):
            wide = pl.ds(pl.multiple_of(block * TB, TB), TB + 32)
            vg[i] = vd[wide, :] + jnp.dot(bk[wide, :], wt[...], preferred_element_type=F32)
        for i, block in enumerate(blocks):
            at = pl.multiple_of(block * TB, TB)
            here = vg[i, 16 : 16 + TB, :]
            total = here * taps[2]
            for j in (0, 1, 3):
                total = total + vg[i, 18 - j : 18 - j + TB, :] * taps[j]
            go[pl.ds(at, TB), :] = total.astype(BF16)
            sums = tuple(
                sums[j]
                + jnp.sum((xf[pl.ds(at + 6 + j, TB), :] * here).reshape(TB // 8, 8, TB), axis=0)
                for j in range(4)
            )
        return sums

    sums = (start,) * 4
    finished = set()
    for turn in (0, 1, 3, 2) if n // batch == 4 else range(n // batch):
        first = n // 2 - batch // 2 + batch * turn
        fresh = [r % n for r in range(first - 1, first + batch + 1)]
        fresh = sorted(set(fresh) - finished)
        finished.update(fresh)
        for r in fresh:
            finish_block(lax.rem(me + r, n))
        apart = [r % n for r in range(first, first + batch)]
        sums = input_grad([lax.rem(me + r, n) for r in apart], sums)
        for r in sorted(apart, key=lambda r: -min(r, n - r)):
            if r:
                outward(lax.rem(me + r, n)).start()

    own_out = pltpu.make_async_copy(rows_of(go, me), columns(gi_ref, me), local_sem.at[2])
    own_out.start()

    maps = jnp.dot(vt[...], bk[16 : length + 16, :], preferred_element_type=F32)
    half = 512 // nc
    third = half // nx
    piece = third // ny
    tap_rows = [jnp.sum(s, axis=0, keepdims=True) for s in sums]
    tile = jnp.concatenate(tap_rows + [jnp.zeros((4, TB), F32)], axis=0)
    for j, column in enumerate((0, 2, 1, 3)):
        c, low = 128 * j // half, 128 * j % half
        halves[c, low : low + 128, :] = maps[:, 128 * column : 128 * column + 128]
    for c in range(nc):
        halves[c, half : half + 8, :] = tile

    def exchange(source, target, device, k):
        return pltpu.make_async_remote_copy(
            src_ref=source,
            dst_ref=target,
            send_sem=r_send.at[k],
            recv_sem=r_recv.at[k],
            device_id=device,
            device_id_type=MESH,
        )

    sent = []

    @pl.when(me > 0)
    def _():
        pl.semaphore_wait(joined.at[1], 1)

    def stage(copies, landing):
        if not copies:
            return
        for copy in copies:
            copy.start()
        k = len(sent)
        whole = landing.at[pl.ds(0, len(copies))]
        sent.append(pltpu.make_async_copy(whole, whole, r_send.at[k]))
        pltpu.make_async_copy(whole, whole, r_recv.at[k]).wait()

    stage([exchange(halves.at[1 - core], core_in.at[0], partner, len(sent))], core_in)
    mine = halves[pl.ds(core, 1)][0] + core_in[0]
    for j in range(nx):
        x_out[j, 0:third, :] = mine[third * j : third * (j + 1)]
        x_out[j, third : third + 8, :] = mine[half : half + 8]
    x_in[pl.ds(xi, 1)] = x_out[pl.ds(xi, 1)]
    stage(
        [
            exchange(x_out.at[p], x_in.at[xi], at_plane(yi, p, core), len(sent))
            for p in x_peers
        ],
        x_in,
    )
    mine = x_in[0]
    for j in range(1, nx):
        mine = mine + x_in[j]
    for j in range(ny):
        y_out[j, 0:piece, :] = mine[piece * j : piece * (j + 1)]
        y_out[j, piece : piece + 8, :] = mine[third : third + 8]
    y_in[pl.ds(yi, 1)] = y_out[pl.ds(yi, 1)]
    stage(
        [
            exchange(y_out.at[p], y_in.at[yi], at_plane(p, xi, core), len(sent))
            for p in y_peers
        ],
        y_in,
    )
    mine = y_in[0]
    for j in range(1, ny):
        mine = mine + y_in[j]
    mine = mine * norm
    gt_ref[...] = mine[piece : piece + 4]
    g2[pl.ds(yi, 1)] = mine[0:piece].reshape(1, piece, TB)
    stage(
        [
            exchange(g2.at[yi], g2.at[yi], at_plane(p, xi, core), len(sent))
            for p in y_peers
        ],
        g2,
    )
    g1[pl.ds(xi, 1)] = g2[...].reshape(1, third, TB)
    stage(
        [
            exchange(g1.at[xi], g1.at[xi], at_plane(yi, p, core), len(sent))
            for p in x_peers
        ],
        g1,
    )
    g0[pl.ds(core, 1)] = g1[...].reshape(1, half, TB)
    stage([exchange(g0.at[core], g0.at[core], partner, len(sent))], g0)
    whole = g0[...].reshape(512, TB)
    for d in range(2):
        gr_ref[d, 0] = whole[128 * d : 128 * d + 128]
        gm_ref[d, 0] = whole[256 + 128 * d : 384 + 128 * d]

    own_out.wait()
    wait_for_blocks(o_recv, n - 1)
    for _ in range(3):
        wait_for_blocks(z_send, n - 1)
    for copy in sent:
        copy.wait()


def store(*refs):
    count = len(refs) // 2
    sems = refs[-1]
    copies = [
        pltpu.make_async_copy(refs[j], refs[count + j], sems.at[j]) for j in range(count)
    ]
    for copy in copies:
        copy.start()
    for copy in copies:
        copy.wait()


def body(sizes, x, cotangent, taps, rate_map, gate_map, logit, spike):
    n, ny, nx, nc, _ = sizes
    length = n * TB
    half, third, piece = 512 // nc, 512 // nc // nx, 512 // nc // nx // ny
    vmem, hbm = pl.BlockSpec(memory_space=pltpu.VMEM), pl.BlockSpec(memory_space=pl.ANY)
    results = pl.pallas_call(
        functools.partial(kernel, sizes),
        name="recurrence_backward",
        out_shape=(
            pltpu.VMEM(x.shape, BF16),
            pltpu.VMEM(rate_map.shape, F32),
            pltpu.VMEM(gate_map.shape, F32),
            pltpu.VMEM(taps.shape, F32),
        ),
        in_specs=[hbm] * 7,
        out_specs=(vmem,) * 4,
        scratch_shapes=[
            pltpu.VMEM(taps.shape, BF16),
            pltpu.VMEM(rate_map.shape, BF16),
            pltpu.VMEM(gate_map.shape, BF16),
            pltpu.VMEM(logit.shape, F32),
            pltpu.VMEM((n, TB), F32),
            pltpu.VMEM((TB, length), BF16),
            pltpu.VMEM((TB, length), BF16),
            pltpu.VMEM((length, TB), BF16),
            pltpu.VMEM((length, TB), BF16),
            pltpu.VMEM((length + 16, TB), F32),
            pltpu.VMEM((length, TB), BF16),
            pltpu.VMEM((TB, length), BF16),
            pltpu.VMEM((TB, 512), BF16),
            pltpu.VMEM((512, TB), BF16),
            pltpu.VMEM((length, 512), F32),
            pltpu.VMEM((2, length + 16, TB), F32),
            pltpu.VMEM((2, length, TB), F32),
            pltpu.VMEM((2, length, TB), F32),
            pltpu.VMEM((2, length, TB), F32),
            pltpu.VMEM((2, length, TB), F32),
            pltpu.VMEM((2, length, TB), F32),
            pltpu.VMEM((2, 4, length, TB), F32),
            pltpu.VMEM((2, length, TB), F32),
            pltpu.VMEM((2, 2, 8 * n, TB), F32),
            pltpu.VMEM((2, 8 * n, TB), F32),
            pltpu.VMEM((2, length, TB), F32),
            pltpu.VMEM((length + 32, TB), F32),
            pltpu.VMEM((min(4, n), TB + 32, TB), F32),
            pltpu.VMEM((length + 32, 512), BF16),
            pltpu.VMEM((length, TB), BF16),
            pltpu.VMEM((nc, half + 8, TB), F32),
            pltpu.VMEM((1, half + 8, TB), F32),
            pltpu.VMEM((nx, third + 8, TB), F32),
            pltpu.VMEM((nx, third + 8, TB), F32),
            pltpu.VMEM((ny, piece + 8, TB), F32),
            pltpu.VMEM((ny, piece + 8, TB), F32),
            pltpu.VMEM((ny, piece, TB), F32),
            pltpu.VMEM((nx, third, TB), F32),
            pltpu.VMEM((nc, half, TB), F32),
            pltpu.SemaphoreType.DMA((3,)),
            pltpu.SemaphoreType.DMA((5,)),
            pltpu.SemaphoreType.DMA,
            pltpu.SemaphoreType.DMA,
            pltpu.SemaphoreType.DMA((n // 2,)),
            pltpu.SemaphoreType.DMA,
            pltpu.SemaphoreType.DMA((6,)),
            pltpu.SemaphoreType.DMA((6,)),
            pltpu.SemaphoreType.REGULAR((2,)),
        ],
        compiler_params=pltpu.CompilerParams(
            collective_id=0, has_side_effects=True, vmem_limit_bytes=56 * 1024 * 1024
        ),
    )(x, cotangent, taps, rate_map, gate_map, logit, spike.reshape(n, TB))
    return pl.pallas_call(
        store,
        name="store_results",
        out_shape=tuple(jax.ShapeDtypeStruct(r.shape, r.dtype) for r in results),
        in_specs=[vmem] * 4,
        out_specs=(hbm,) * 4,
        scratch_shapes=[pltpu.SemaphoreType.DMA((4,))],
    )(*[pltpu.with_memory_space_constraint(r, pltpu.VMEM) for r in results])


def solution(mesh):
    n, dp = mesh.shape["sp"], mesh.shape["dp"]
    ny, nx, nc = grid_of(dp)
    sizes = (n, ny, nx, nc, 1.0 / math.sqrt(dp * n * TB))
    return jax.shard_map(
        functools.partial(body, sizes),
        mesh=mesh,
        in_specs=(
            P("dp", "sp", None),
            P("dp", "sp", None),
            P(None, "sp"),
            P(None, "sp", None, None),
            P(None, "sp", None, None),
            P(None, "sp"),
            P("dp", "sp", None),
        ),
        out_specs=(
            P("dp", "sp", None),
            P(None, "sp", None, None),
            P(None, "sp", None, None),
            P(None, "sp"),
        ),
        check_vma=False,
    )
```

```python
import functools
import math

import jax
import jax.numpy as jnp
from jax import lax
from jax.experimental import pallas as pl
from jax.experimental.pallas import tpu as pltpu
from jax.sharding import PartitionSpec as P

MESH = pl.DeviceIdType.MESH
TB = 128
F32 = jnp.float32
BF16 = jnp.bfloat16
STRENGTH = 8.0


def grid_of(dp):
    return (8, 4, 2) if dp == 64 else (dp // 4, 2, 2)


def log_keep_of(logit):
    u = jnp.exp(-jnp.abs(logit))
    series = u * (1.0 - u * (0.5 - u * (1.0 / 3.0 - u * 0.25)))
    return jnp.minimum(logit, 0.0) - jnp.where(u < 0.01, series, jnp.log(1.0 + u))


def sigmoid(x):
    return 1.0 / (1.0 + jnp.exp(-x))


def one_less_square(log_decay, decay):
    y = -2.0 * log_decay
    series = y * (1.0 - y * (0.5 - y * (1.0 / 6.0 - y * (1.0 / 24.0 - y * (1.0 / 120.0)))))
    return jnp.where(y < 0.125, series, 1.0 - decay * decay)


def shifted(value, step, forward):
    return pltpu.roll(value, step if forward else 8 - step, 1)


def prefixes(coeff, row, forward):
    outs, product = [], coeff
    for step in (1, 2, 4):
        inside = (row >= step) if forward else (row < 8 - step)
        outs.append(jnp.where(inside, product, 0.0))
        product = jnp.where(inside, product * shifted(product, step, forward), product)
    return outs, product


def doubled(value, steps, forward):
    for step, coeff in zip((1, 2, 4), steps):
        value = value + coeff * shifted(value, step, forward)
    return value


def last_row(value, forward):
    edge = value[7:8] if forward else value[0:1]
    return jnp.broadcast_to(edge, value.shape)


def kernel(
    sizes,
    x_hbm,
    cot_hbm,
    taps_hbm,
    wr_hbm,
    wi_hbm,
    logit_hbm,
    spike_hbm,
    gi_ref,
    gr_ref,
    gm_ref,
    gt_ref,
    taps_ref,
    wr_ref,
    wi_ref,
    logit_ref,
    spike_ref,
    xs,
    cs,
    xr,
    cr,
    xf,
    vs,
    vt,
    wcat,
    wt,
    pre,
    af,
    sc,
    e1,
    e2,
    c2,
    c3,
    qs,
    gs,
    ends,
    carries,
    zs,
    vd,
    vg,
    bk,
    go,
    halves,
    core_in,
    x_out,
    x_in,
    y_out,
    y_in,
    g2,
    g1,
    g0,
    local_sem,
    small_sem,
    z_send,
    x_recv,
    c_recv,
    o_recv,
    r_send,
    r_recv,
    joined,
):
    n, ny, nx, nc, norm = sizes
    length = n * TB
    me = lax.axis_index("sp")
    dp = lax.axis_index("dp")
    core = lax.rem(dp, nc)
    xi = lax.rem(dp // nc, nx)
    yi = dp // (nc * nx)

    def at_plane(y, x, c):
        return {"sp": me, "dp": (y * nx + x) * nc + c}

    def along_z(peer):
        return {"sp": peer, "dp": dp}

    offsets = [n // 2]
    for d in range(n // 2 - 1, 0, -1):
        offsets += [d, n - d]
    x_peers = [lax.rem(xi + d, nx) for d in range(1, nx)]
    y_peers = [lax.rem(yi + d, ny) for d in range(1, ny)]
    partner = at_plane(yi, xi, 1 - core)

    barrier = pltpu.get_barrier_semaphore()
    column = [along_z(lax.rem(me + d, n)) for d in offsets]
    plane = [at_plane(yi, x, core) for x in x_peers]
    plane += [at_plane(y, xi, core) for y in y_peers]
    plane += [partner]
    for device in column:
        pl.semaphore_signal(barrier, inc=1, device_id=device, device_id_type=MESH)

    @pl.when(me == 0)
    def _():
        for device in plane:
            pl.semaphore_signal(barrier, inc=1, device_id=device, device_id_type=MESH)

    def columns(ref, block):
        return ref.at[0, :, pl.ds(pl.multiple_of(block * TB, TB), TB)]

    def rows_of(ref, block):
        return ref.at[pl.ds(pl.multiple_of(block * TB, TB), TB)]

    own = [
        pltpu.make_async_copy(x_hbm.at[0], xs, local_sem.at[0]),
        pltpu.make_async_copy(cot_hbm.at[0], cs, local_sem.at[1]),
    ]
    own[0].start()
    own[1].start()
    small = [
        pltpu.make_async_copy(source, target, small_sem.at[j])
        for j, (source, target) in enumerate(
            (
                (taps_hbm, taps_ref),
                (wr_hbm, wr_ref),
                (wi_hbm, wi_ref),
                (logit_hbm, logit_ref),
                (spike_hbm, spike_ref),
            )
        )
    ]
    for copy in small:
        copy.start()

    @pl.when(me > 0)
    def _():
        pl.semaphore_wait(barrier, len(column))

    @pl.when(me == 0)
    def _():
        pl.semaphore_wait(barrier, len(column) + len(plane))


    def inward(which, k):
        source, target = ((xs, xr), (cs, cr))[which]
        peer = lax.rem(me + offsets[k], n)
        return pltpu.make_async_remote_copy(
            src_ref=source.at[:, pl.ds(pl.multiple_of(peer * TB, TB), TB)],
            dst_ref=rows_of(target, me),
            send_sem=z_send,
            recv_sem=x_recv if which == 0 else c_recv.at[(k + 1) // 2],
            device_id=along_z(peer),
            device_id_type=MESH,
        )

    def pair(j):
        near = n // 2 - j
        later = (j + n // 2 - 1) // (n // 2)
        return lax.rem(me + near, n), lax.rem(me + n - near * later, n)

    def wait_for_blocks(sem, count):
        rows = pl.ds(0, count * TB)
        pltpu.make_async_copy(xr.at[rows], xr.at[rows], sem).wait()

    mine = pl.ds(pl.multiple_of(me * TB, TB), TB)
    for which, (source, target) in enumerate(((xs, xr), (cs, cr))):
        own[which].wait()
        for k in range(n - 1):
            inward(which, k).start()
        target[mine, :] = source[:, mine]

    for copy in small:
        copy.wait()
    zero_rows = jnp.zeros((8, TB), F32)
    xf[0:8, :] = zero_rows
    xf[length + 8 : length + 16, :] = zero_rows
    for edge in (0, length + 16):
        vd[edge : edge + 16, :] = jnp.zeros((16, TB), F32)
        bk[edge : edge + 16, :] = jnp.zeros((16, 512), BF16)
    for d in range(2):
        af[d, 0:8, :] = zero_rows
        af[d, length + 8 : length + 16, :] = zero_rows
        wcat[:, 256 * d : 256 * d + 128] = wr_ref[d, 0]
        wcat[:, 256 * d + 128 : 256 * d + 256] = wi_ref[d, 0]
        for j, ref in enumerate((wr_ref, wi_ref)):
            flipped = jnp.transpose(ref[d, 0].astype(F32)).astype(BF16)
            wt[256 * d + 128 * j : 256 * d + 128 * j + 128, :] = flipped
    taps = [taps_ref[k : k + 1, :].astype(F32) for k in range(4)]
    keep = [STRENGTH * log_keep_of(logit_ref[d : d + 1, :]) for d in range(2)]
    row = lax.broadcasted_iota(jnp.int32, (8, 8, TB), 1)
    row0 = lax.broadcasted_iota(jnp.int32, (8, TB), 0)

    wait_for_blocks(x_recv, n - 1)

    @pl.when(me == 0)
    def _():
        for device in plane:
            pl.semaphore_signal(joined.at[0], inc=1, device_id=device, device_id_type=MESH)


    @pl.loop(0, n)
    def _(b):
        at = pl.multiple_of(b * TB, TB)
        xf[pl.ds(at + 8, TB), :] = xr[pl.ds(at, TB), :].astype(F32)

    @pl.loop(0, n)
    def _(b):
        at = pl.multiple_of(b * TB, TB)
        v = xf[pl.ds(at + 6, TB), :] * taps[0]
        for k in range(1, 4):
            v = v + xf[pl.ds(at + 6 + k, TB), :] * taps[k]
        low = v.astype(BF16)
        vs[pl.ds(at, TB), :] = low
        vt[:, pl.ds(at, TB)] = jnp.transpose(low.astype(F32)).astype(BF16)

    chunk = min(512, length)

    @pl.loop(0, length // chunk)
    def _(b):
        at = pl.multiple_of(b * chunk, chunk)
        pre[pl.ds(at, chunk), :] = jnp.dot(
            vs[pl.ds(at, chunk), :], wcat[...], preferred_element_type=F32
        )

    @pl.loop(0, n)
    def _(b):
        at = pl.multiple_of(b * TB, TB)
        spike = jnp.transpose(jnp.broadcast_to(spike_ref[pl.ds(b, 1), :], (TB, TB)))
        v = vs[pl.ds(at, TB), :].astype(F32)
        for d in range(2):
            rate = sigmoid(pre[pl.ds(at, TB), 256 * d : 256 * d + 128])
            gate = sigmoid(pre[pl.ds(at, TB), 256 * d + 128 : 256 * d + 256])
            log_decay = rate * keep[d] + spike
            decay = jnp.exp(log_decay)
            square = one_less_square(log_decay, decay)
            inverse = lax.rsqrt(square)
            multiplier = square * inverse
            gated = gate * v
            source = multiplier * gated
            slope = keep[d] * rate * (1.0 - rate)
            sloped = decay * slope
            af[d, pl.ds(at + 8, TB), :] = decay
            sc[d, pl.ds(at, TB), :] = source
            e1[d, pl.ds(at, TB), :] = sloped
            e2[d, pl.ds(at, TB), :] = -gated * decay * sloped * inverse
            c2[d, pl.ds(at, TB), :] = source * (1.0 - gate)
            c3[d, pl.ds(at, TB), :] = multiplier * gate

    def state_pass(d, block, carry):
        forward = d == 0
        at = pl.multiple_of(block * 64, 64)
        coeff = af[d, pl.ds(at + 8, 64), :].reshape(8, 8, TB)
        steps, product = prefixes(coeff, row, forward)
        value = doubled(sc[d, pl.ds(at, 64), :].reshape(8, 8, TB), steps, forward)
        for g in range(8) if forward else range(7, -1, -1):
            state = value[g] + product[g] * carry
            edge = (row0 == 0) if forward else (row0 == 7)
            before = jnp.where(edge, carry, pltpu.roll(state, 1 if forward else 7, 0))
            spot = pl.ds(at + 8 * g, 8)
            e1[d, spot, :] = before * e1[d, spot, :] + e2[d, spot, :]
            carry = last_row(state, forward)
        return carry

    def state_step(i, carry):
        ahead = state_pass(0, i, carry[0])
        back = state_pass(1, length // 64 - 1 - i, carry[1])
        return ahead, back

    start = jnp.zeros((8, TB), F32)
    lax.fori_loop(0, length // 64, state_step, (start, start))

    @pl.loop(0, n)
    def _(b):
        at = pl.multiple_of(b * TB, TB)
        for d in range(2):
            forward = d == 1
            shift = -1 if forward else 1
            carry = jnp.ones((8, TB), F32)
            for part in (0, 1) if forward else (1, 0):
                coeff = af[d, pl.ds(at + 64 * part + 8 + shift, 64), :].reshape(8, 8, TB)
                steps, product = prefixes(coeff, row, forward)
                for j, step in enumerate(steps):
                    qs[d, j, pl.ds(at + 64 * part, 64), :] = step.reshape(64, TB)
                qs[d, 3, pl.ds(at + 64 * part, 64), :] = product.reshape(64, TB)
                for g in range(8) if forward else range(7, -1, -1):
                    whole = product[g] * carry
                    gs[d, pl.ds(at + 64 * part + 8 * g, 8), :] = whole
                    carry = last_row(whole, forward)
            ends[d, 0, pl.ds(pl.multiple_of(b * 8, 8), 8), :] = carry

    def local_scan(d, block):
        forward = d == 1
        at = pl.multiple_of(block * TB, TB)
        carry = None
        for part in (0, 1) if forward else (1, 0):
            spot = pl.ds(at + 64 * part, 64)
            steps = [qs[d, j, spot, :].reshape(8, 8, TB) for j in range(3)]
            value = doubled(cr[spot, :].astype(F32).reshape(8, 8, TB), steps, forward)
            product = qs[d, 3, spot, :].reshape(8, 8, TB)
            for g in range(8) if forward else range(7, -1, -1):
                adjoint = value[g] if carry is None else value[g] + product[g] * carry
                zs[d, pl.ds(at + 64 * part + 8 * g, 8), :] = adjoint
                carry = last_row(adjoint, forward)
        ends[d, 1, pl.ds(pl.multiple_of(block * 8, 8), 8), :] = carry

    @pl.when(me == 0)
    def _():
        pl.semaphore_wait(joined.at[0], len(plane))
        for device in column:
            pl.semaphore_signal(joined.at[1], inc=1, device_id=device, device_id_type=MESH)

    def scan_pair(j):
        for block in pair(j):
            local_scan(0, block)
            local_scan(1, block)

    wait_for_blocks(c_recv.at[0], 1)
    scan_pair(0)

    @pl.loop(1, n // 2)
    def _(j):
        wait_for_blocks(c_recv.at[j], 2)
        scan_pair(j)

    ahead = back = start
    for b in range(n):
        carries[1, 8 * b : 8 * b + 8, :] = ahead
        ahead = ends[1, 1, 8 * b : 8 * b + 8, :] + ends[1, 0, 8 * b : 8 * b + 8, :] * ahead
        r = n - 1 - b
        carries[0, 8 * r : 8 * r + 8, :] = back
        back = ends[0, 1, 8 * r : 8 * r + 8, :] + ends[0, 0, 8 * r : 8 * r + 8, :] * back

    def finish_block(b):
        incoming = [carries[d, pl.ds(pl.multiple_of(b * 8, 8), 8), :] for d in range(2)]
        for part in range(4):
            at = pl.multiple_of(b * TB + 32 * part, 32)
            spot, padded = pl.ds(at, 32), pl.ds(at + 16, 32)
            total = None
            for d in range(2):
                local = zs[d, spot, :].reshape(4, 8, TB)
                spread = gs[d, spot, :].reshape(4, 8, TB) * incoming[d][None]
                adjoint = (local + spread).reshape(32, TB)
                bk[padded, 256 * d : 256 * d + 128] = (adjoint * e1[d, spot, :]).astype(BF16)
                bk[padded, 256 * d + 128 : 256 * d + 256] = (adjoint * c2[d, spot, :]).astype(BF16)
                direct = adjoint * c3[d, spot, :]
                total = direct if total is None else total + direct
            vd[padded, :] = total

    def outward(block):
        return pltpu.make_async_remote_copy(
            src_ref=rows_of(go, block),
            dst_ref=columns(gi_ref, me),
            send_sem=z_send,
            recv_sem=o_recv,
            device_id=along_z(block),
            device_id_type=MESH,
        )

    batch = min(4, n)

    def input_grad(blocks, away, sums):
        for i, block in enumerate(blocks):
            wide = pl.ds(pl.multiple_of(block * TB, TB), TB + 32)
            vg[i] = vd[wide, :] + jnp.dot(bk[wide, :], wt[...], preferred_element_type=F32)
        for i, block in enumerate(blocks):
            at = pl.multiple_of(block * TB, TB)
            here = vg[i, 16 : 16 + TB, :]
            total = here * taps[2]
            for j in (0, 1, 3):
                total = total + vg[i, 18 - j : 18 - j + TB, :] * taps[j]
            go[pl.ds(at, TB), :] = total.astype(BF16)
            if away[i]:
                outward(block).start()
            sums = tuple(
                sums[j]
                + jnp.sum((xf[pl.ds(at + 6 + j, TB), :] * here).reshape(TB // 8, 8, TB), axis=0)
                for j in range(4)
            )
        return sums

    sums = (start,) * 4
    finished = set()
    for turn in (0, 1, 3, 2) if n // batch == 4 else range(n // batch):
        first = n // 2 - batch // 2 + batch * turn
        fresh = [r % n for r in range(first - 1, first + batch + 1)]
        fresh = sorted(set(fresh) - finished)
        finished.update(fresh)
        for r in fresh:
            finish_block(lax.rem(me + r, n))
        apart = [r % n for r in range(first, first + batch)]
        apart = sorted(apart, key=lambda r: -min(r, n - r))
        sums = input_grad([lax.rem(me + r, n) for r in apart], apart, sums)

    own_out = pltpu.make_async_copy(rows_of(go, me), columns(gi_ref, me), local_sem.at[2])
    own_out.start()

    maps = jnp.dot(vt[...], bk[16 : length + 16, :], preferred_element_type=F32)
    half = 512 // nc
    third = half // nx
    piece = third // ny
    tap_rows = [jnp.sum(s, axis=0, keepdims=True) for s in sums]
    tile = jnp.concatenate(tap_rows + [jnp.zeros((4, TB), F32)], axis=0)
    for j, column in enumerate((0, 2, 1, 3)):
        c, low = 128 * j // half, 128 * j % half
        halves[c, low : low + 128, :] = maps[:, 128 * column : 128 * column + 128]
    for c in range(nc):
        halves[c, half : half + 8, :] = tile

    def exchange(source, target, device, k):
        return pltpu.make_async_remote_copy(
            src_ref=source,
            dst_ref=target,
            send_sem=r_send.at[k],
            recv_sem=r_recv.at[k],
            device_id=device,
            device_id_type=MESH,
        )

    sent = []

    @pl.when(me > 0)
    def _():
        pl.semaphore_wait(joined.at[1], 1)

    def stage(copies, landing):
        if not copies:
            return
        for copy in copies:
            copy.start()
        k = len(sent)
        whole = landing.at[pl.ds(0, len(copies))]
        sent.append(pltpu.make_async_copy(whole, whole, r_send.at[k]))
        pltpu.make_async_copy(whole, whole, r_recv.at[k]).wait()

    stage([exchange(halves.at[1 - core], core_in.at[0], partner, len(sent))], core_in)
    mine = halves[pl.ds(core, 1)][0] + core_in[0]
    for j in range(nx):
        x_out[j, 0:third, :] = mine[third * j : third * (j + 1)]
        x_out[j, third : third + 8, :] = mine[half : half + 8]
    x_in[pl.ds(xi, 1)] = x_out[pl.ds(xi, 1)]
    stage(
        [
            exchange(x_out.at[p], x_in.at[xi], at_plane(yi, p, core), len(sent))
            for p in x_peers
        ],
        x_in,
    )
    mine = x_in[0]
    for j in range(1, nx):
        mine = mine + x_in[j]
    for j in range(ny):
        y_out[j, 0:piece, :] = mine[piece * j : piece * (j + 1)]
        y_out[j, piece : piece + 8, :] = mine[third : third + 8]
    y_in[pl.ds(yi, 1)] = y_out[pl.ds(yi, 1)]
    stage(
        [
            exchange(y_out.at[p], y_in.at[yi], at_plane(p, xi, core), len(sent))
            for p in y_peers
        ],
        y_in,
    )
    mine = y_in[0]
    for j in range(1, ny):
        mine = mine + y_in[j]
    mine = mine * norm
    gt_ref[...] = mine[piece : piece + 4]
    g2[pl.ds(yi, 1)] = mine[0:piece].reshape(1, piece, TB)
    stage(
        [
            exchange(g2.at[yi], g2.at[yi], at_plane(p, xi, core), len(sent))
            for p in y_peers
        ],
        g2,
    )
    g1[pl.ds(xi, 1)] = g2[...].reshape(1, third, TB)
    stage(
        [
            exchange(g1.at[xi], g1.at[xi], at_plane(yi, p, core), len(sent))
            for p in x_peers
        ],
        g1,
    )
    g0[pl.ds(core, 1)] = g1[...].reshape(1, half, TB)
    stage([exchange(g0.at[core], g0.at[core], partner, len(sent))], g0)
    whole = g0[...].reshape(512, TB)
    for d in range(2):
        gr_ref[d, 0] = whole[128 * d : 128 * d + 128]
        gm_ref[d, 0] = whole[256 + 128 * d : 384 + 128 * d]

    own_out.wait()
    wait_for_blocks(o_recv, n - 1)
    for _ in range(3):
        wait_for_blocks(z_send, n - 1)
    for copy in sent:
        copy.wait()


def store(*refs):
    count = len(refs) // 2
    sems = refs[-1]
    copies = [
        pltpu.make_async_copy(refs[j], refs[count + j], sems.at[j]) for j in range(count)
    ]
    for copy in copies:
        copy.start()
    for copy in copies:
        copy.wait()


def body(sizes, x, cotangent, taps, rate_map, gate_map, logit, spike):
    n, ny, nx, nc, _ = sizes
    length = n * TB
    half, third, piece = 512 // nc, 512 // nc // nx, 512 // nc // nx // ny
    vmem, hbm = pl.BlockSpec(memory_space=pltpu.VMEM), pl.BlockSpec(memory_space=pl.ANY)
    results = pl.pallas_call(
        functools.partial(kernel, sizes),
        name="recurrence_backward",
        out_shape=(
            pltpu.VMEM(x.shape, BF16),
            pltpu.VMEM(rate_map.shape, F32),
            pltpu.VMEM(gate_map.shape, F32),
            pltpu.VMEM(taps.shape, F32),
        ),
        in_specs=[hbm] * 7,
        out_specs=(vmem,) * 4,
        scratch_shapes=[
            pltpu.VMEM(taps.shape, BF16),
            pltpu.VMEM(rate_map.shape, BF16),
            pltpu.VMEM(gate_map.shape, BF16),
            pltpu.VMEM(logit.shape, F32),
            pltpu.VMEM((n, TB), F32),
            pltpu.VMEM((TB, length), BF16),
            pltpu.VMEM((TB, length), BF16),
            pltpu.VMEM((length, TB), BF16),
            pltpu.VMEM((length, TB), BF16),
            pltpu.VMEM((length + 16, TB), F32),
            pltpu.VMEM((length, TB), BF16),
            pltpu.VMEM((TB, length), BF16),
            pltpu.VMEM((TB, 512), BF16),
            pltpu.VMEM((512, TB), BF16),
            pltpu.VMEM((length, 512), F32),
            pltpu.VMEM((2, length + 16, TB), F32),
            pltpu.VMEM((2, length, TB), F32),
            pltpu.VMEM((2, length, TB), F32),
            pltpu.VMEM((2, length, TB), F32),
            pltpu.VMEM((2, length, TB), F32),
            pltpu.VMEM((2, length, TB), F32),
            pltpu.VMEM((2, 4, length, TB), F32),
            pltpu.VMEM((2, length, TB), F32),
            pltpu.VMEM((2, 2, 8 * n, TB), F32),
            pltpu.VMEM((2, 8 * n, TB), F32),
            pltpu.VMEM((2, length, TB), F32),
            pltpu.VMEM((length + 32, TB), F32),
            pltpu.VMEM((min(4, n), TB + 32, TB), F32),
            pltpu.VMEM((length + 32, 512), BF16),
            pltpu.VMEM((length, TB), BF16),
            pltpu.VMEM((nc, half + 8, TB), F32),
            pltpu.VMEM((1, half + 8, TB), F32),
            pltpu.VMEM((nx, third + 8, TB), F32),
            pltpu.VMEM((nx, third + 8, TB), F32),
            pltpu.VMEM((ny, piece + 8, TB), F32),
            pltpu.VMEM((ny, piece + 8, TB), F32),
            pltpu.VMEM((ny, piece, TB), F32),
            pltpu.VMEM((nx, third, TB), F32),
            pltpu.VMEM((nc, half, TB), F32),
            pltpu.SemaphoreType.DMA((3,)),
            pltpu.SemaphoreType.DMA((5,)),
            pltpu.SemaphoreType.DMA,
            pltpu.SemaphoreType.DMA,
            pltpu.SemaphoreType.DMA((n // 2,)),
            pltpu.SemaphoreType.DMA,
            pltpu.SemaphoreType.DMA((6,)),
            pltpu.SemaphoreType.DMA((6,)),
            pltpu.SemaphoreType.REGULAR((2,)),
        ],
        compiler_params=pltpu.CompilerParams(
            collective_id=0, has_side_effects=True, vmem_limit_bytes=56 * 1024 * 1024
        ),
    )(x, cotangent, taps, rate_map, gate_map, logit, spike.reshape(n, TB))
    return pl.pallas_call(
        store,
        name="store_results",
        out_shape=tuple(jax.ShapeDtypeStruct(r.shape, r.dtype) for r in results),
        in_specs=[vmem] * 4,
        out_specs=(hbm,) * 4,
        scratch_shapes=[pltpu.SemaphoreType.DMA((4,))],
    )(*[pltpu.with_memory_space_constraint(r, pltpu.VMEM) for r in results])


def solution(mesh):
    n, dp = mesh.shape["sp"], mesh.shape["dp"]
    ny, nx, nc = grid_of(dp)
    sizes = (n, ny, nx, nc, 1.0 / math.sqrt(dp * n * TB))
    return jax.shard_map(
        functools.partial(body, sizes),
        mesh=mesh,
        in_specs=(
            P("dp", "sp", None),
            P("dp", "sp", None),
            P(None, "sp"),
            P(None, "sp", None, None),
            P(None, "sp", None, None),
            P(None, "sp"),
            P("dp", "sp", None),
        ),
        out_specs=(
            P("dp", "sp", None),
            P(None, "sp", None, None),
            P(None, "sp", None, None),
            P(None, "sp"),
        ),
        check_vma=False,
    )
```
